32 devices in a mesh: sp: 4 (over y, x), tp: 8 (over z, core).
Axes of the slice: x: 2, y: 2, z: 4, core: 2. Of those that a mesh axis runs over, the one named last changes fastest.
Arguments:
- residual_mid: bfloat16 [640, 4096], P('sp'), may hold values from -100 to 100
- out_grad: bfloat16 [640, 4096], P('sp'), may hold values from -6 to 6
- norm_gain: float32 [4096], replicated, may hold values from 0.1 to 1.9
- expert_ids: int32 [640, 2], P('sp'), may hold values from 0 to 3, all different within a row; in each aligned block of 160 rows (0 to 159, 160 to 319, ...) at most 160 rows name the same one
- expert_weights: float32 [640, 2], P('sp'), may hold values from 0.1 to 1
- gate_proj: bfloat16 [4, 4096, 2048], P('sp', None, 'tp'), may hold values from -0.25 to 0.25
- up_proj: bfloat16 [4, 4096, 2048], P('sp', None, 'tp'), may hold values from -0.25 to 0.25
- down_proj: bfloat16 [4, 2048, 4096], P('sp', 'tp'), may hold values from -0.125 to 0.125
- out_proj: bfloat16 [4096, 4096], P('tp'), may hold values from -0.09375 to 0.09375
- query_rows: bfloat16 [640, 4096], P('sp', 'tp'), may hold values from -6 to 6
- key_rows: bfloat16 [640, 4096], P('sp', 'tp'), may hold values from -6 to 6
- value_rows: bfloat16 [640, 4096], P('sp', 'tp'), may hold values from -6 to 6
- retention_out: bfloat16 [640, 4096], P('sp', 'tp'), may hold values from -6 to 6
- log_decay: float32 [640, 16], P('sp', 'tp'), may hold values from -2 to 0
- entry_state: float32 [4, 16, 256, 256], P('sp', 'tp'), may hold values from -24 to 24
Outputs:
- gate_grad: bfloat16 [4, 4096, 2048], P('sp', None, 'tp')
- up_grad: bfloat16 [4, 4096, 2048], P('sp', None, 'tp')
- down_grad: bfloat16 [4, 2048, 4096], P('sp', 'tp')
- proj_grad: float32 [4096, 4096], P('sp', 'tp')
- query_grad: bfloat16 [640, 4096], P('sp', 'tp')
- key_grad: bfloat16 [640, 4096], P('sp', 'tp')
- value_grad: bfloat16 [640, 4096], P('sp', 'tp')
The draws below stay inside these ranges and needn't reach their ends.
Inputs may be any that keep to these rules, and one draw needn't show every extreme that they name: `expert_ids`: each row names 2 different experts. Among the rows of one device, no expert is named by more than 160 rows, and in every draw some expert is named by exactly 160 rows of some device.
All inputs are finite; a program needn't handle non-finite values.
Results may differ from the reference program's by a relative error of at most 0.025.
The reference program's roundings to bfloat16 on the way count: a program that leaves them out, or rounds other values in their place, can miss the bound.
Values may be sent and summed in bfloat16 or wider, within the bound.
A program may use at most 128 MiB of HBM per device.

```python
import math
import jax
import jax.numpy as jnp
import numpy as np
from jax import lax

D = 4096
FF = 2048
RETENTION_HEADS = 16
DK = 256
TOP = 2
TOK_DEV = 160
RW = 4096
EXPERTS = 4
SEGS = 4
SEQUENCE_TOKENS = 640
CAP = 160
N_TP = 8


def draw_residual_mid(key, part):
    base_key, col_key, row_key = jax.random.split(key, 3)
    columns = jnp.exp(jax.random.uniform(col_key, (1, D), jnp.float32, 0.0, math.log(10.0)))
    rowscale = jnp.exp(jax.random.uniform(row_key, (SEQUENCE_TOKENS, 1), jnp.float32, math.log(0.3), math.log(3.0)))
    entries = jnp.clip(jax.random.normal(base_key, (SEQUENCE_TOKENS, D), jnp.float32), -6.0, 6.0)
    return (entries * columns * rowscale / 3.0).astype(jnp.bfloat16)


def draw_log_decay(key, part):
    random_keys = jax.random.split(key, 7)
    head_order = jax.random.permutation(random_keys[0], RETENTION_HEADS)
    fast_heads = head_order < RETENTION_HEADS // 2
    fast_span = jnp.exp(jax.random.uniform(random_keys[1], (RETENTION_HEADS,), jnp.float32, math.log(30.0), math.log(100.0)))
    slow_total = jax.random.uniform(random_keys[2], (RETENTION_HEADS,), jnp.float32, 0.05, 0.2) * math.log(10.0)
    decay_speed = jnp.where(fast_heads, math.log(20.0) / fast_span, slow_total / SEQUENCE_TOKENS)
    segment_multiplier = jnp.exp(jax.random.uniform(random_keys[3], (SEGS, RETENTION_HEADS), jnp.float32, math.log(0.5), math.log(2.0)))
    segment_multiplier = jnp.repeat(segment_multiplier, TOK_DEV, axis=0)
    jaggedness = jax.random.uniform(random_keys[4], (SEQUENCE_TOKENS, RETENTION_HEADS), jnp.float32, 0.5, 1.5)
    spike_position = jax.random.randint(random_keys[5], (2, 1), 0, SEQUENCE_TOKENS)
    spike_retained = jax.random.uniform(random_keys[6], (2, RETENTION_HEADS), jnp.float32, 0.5, 0.8)
    token_position = jnp.arange(SEQUENCE_TOKENS)[None, :, None]
    spike_matches = token_position == spike_position[:, :, None]
    spike_list = jnp.sum(jnp.where(spike_matches, jnp.log(spike_retained)[:, None, :], 0.0), axis=0)
    return (-decay_speed[None, :] * segment_multiplier * jaggedness + spike_list).astype(jnp.float32)


def with_spikes(values, own_key, source, target, blocks, factor):
    def block_of(position):
        return (jnp.arange(values.shape[position]) // (values.shape[position] // blocks)).reshape((-1,) + (1,) * (values.ndim - 1 - position))

    one_side = jax.random.permutation(own_key, blocks)[block_of(target)]
    other_side = (block_of(target) + blocks // 2) % blocks
    return jnp.where((block_of(source) == one_side) | (block_of(source) == other_side), factor * values, values)


def block_scale(own_key, shape, shards, least, largest):
    factor_of, own = 1.0, jax.random.fold_in(own_key, 6)
    for position, shards_of in shards:
        draws = jnp.exp(jax.random.uniform(jax.random.fold_in(own, position), (shards_of,), jnp.float32, least / len(shards), largest / len(shards)))
        factor_of = factor_of * jnp.repeat(draws, shape[position] // shards_of).reshape([-1 if axis == position else 1 for axis in range(len(shape))])
    return factor_of


def assign_block(key, own, number, rows, number_of, top, bound, slope):
    sequence = jax.random.permutation(key, number_of)
    packed, usual = portions_of(number_of, rows * top, bound, slope, True), portions_of(number_of, rows * top, bound, slope, False)
    places = jnp.arange(number_of)

    def named(lengths, offset_by):
        used = int((lengths > 0).sum())
        fixed = max(1, used // 4)
        passed = fixed + (places - fixed + offset_by * (used - fixed)) % max(1, number_of - fixed)
        return jnp.zeros((number_of,), jnp.int32).at[sequence[jnp.where(places < fixed, places, passed)]].set(jnp.asarray(lengths, jnp.int32))

    lengths = jnp.where(number % 4 == 0, named(packed, number // 4), named(usual, number - number // 4 - 1))
    mixed = jax.random.permutation(jax.random.fold_in(own, 3), number_of)
    giver, taker = mixed[0:number_of // 2 * 2:2], mixed[1:number_of // 2 * 2:2]
    room = jnp.minimum(lengths[giver] - 1, bound - lengths[taker]) // 2
    room = jnp.where((giver == sequence[0]) | (taker == sequence[0]) | (lengths[taker] == 0), 0, jnp.maximum(room, 0))
    passed = jax.random.randint(jax.random.fold_in(own, 4), (number_of // 2,), 0, 1 << 20) % (room + 1)
    lengths = lengths.at[giver].add(-passed).at[taker].add(passed)
    items = jnp.searchsorted(jnp.cumsum(lengths), jnp.arange(rows * top), side="right").astype(jnp.int32)
    listing = items.reshape(top, rows).T
    listing = listing[jax.random.permutation(jax.random.fold_in(own, 1), rows)]
    offset_by = jax.random.randint(jax.random.fold_in(own, 2), (rows, 1), 0, top)
    return jnp.take_along_axis(listing, (jnp.arange(top)[None, :] + offset_by) % top, axis=1)


def portions_of(amount, total, bound, slope, full):
    weights = [(1 << 20) // math.isqrt(grade ** slope) + 1 for grade in range(1, amount + 1)]
    largest = bound if full else min(bound, max(-(-total // amount), total * weights[0] // sum(weights)))
    least = 1 if total - largest >= amount - 1 else 0
    counts, spare = [largest] + [least] * (amount - 1), total - largest - least * (amount - 1)
    while spare > 0:
        free = [i for i in range(1, amount) if counts[i] < largest] or [i for i in range(1, amount) if counts[i] < bound]
        mass, budget = sum([weights[i] for i in free]), spare
        for i in free:
            extra = min(bound - counts[i], max(1, budget * weights[i] // mass), spare)
            counts[i] = counts[i] + extra
            spare = spare - extra
    return np.array(counts)


def centred(stream_key, extent, scale, bound, cuts=(), kind=jnp.bfloat16):
    level = block_scale(stream_key, extent, cuts, -0.22, 0.18) if cuts else 1.0
    values = jax.random.normal(stream_key, extent, jnp.float32) * scale * level
    return jnp.minimum(jnp.maximum(values, -bound), bound).astype(kind)


def bell_draw_with(stream_key, shape, scale, reach, shards, heavy, kind=jnp.bfloat16):
    result = scale * jax.random.normal(stream_key, shape, jnp.float32)
    if shards:
        result = result * block_scale(stream_key, shape, shards, -0.22, 0.18)
    return jnp.clip(with_spikes(result, jax.random.fold_in(stream_key, 3), *heavy), -reach, reach).astype(kind)


def setup_inputs(seed: int = 0) -> dict:
    keys = jax.random.split(jax.random.key(seed), 16)
    residual_mid = draw_residual_mid(jax.random.fold_in(keys[15], 71), 0)
    out_grad = bell_draw_with(keys[1], (SEQUENCE_TOKENS, D), 1.0, 6.0, ((0, 4),), (0, 1, 4, 2.0))
    norm_gain = jnp.clip(1.0 + 0.18 * jax.random.normal(keys[2], (D,), jnp.float32), 0.1, 1.9)
    expert_ids_keys = jax.random.split(jax.random.fold_in(keys[3], 1), SEQUENCE_TOKENS // TOK_DEV)
    expert_ids_turns = jax.random.permutation(jax.random.fold_in(keys[3], 3), SEQUENCE_TOKENS // TOK_DEV)
    expert_ids = jax.vmap(lambda own, number: assign_block(jax.random.fold_in(keys[3], 2), own, number, TOK_DEV, EXPERTS, TOP, CAP, 2))(expert_ids_keys, expert_ids_turns).reshape((SEQUENCE_TOKENS, TOP))
    expert_weights = jnp.clip(0.1 + 0.9 * jax.random.uniform(keys[4], (SEQUENCE_TOKENS, TOP), jnp.float32) ** block_scale(keys[4], (SEQUENCE_TOKENS, TOP), ((0, 4),), -0.2, 0.2), 0.1, 1.0)
    gate_proj = centred(keys[5], (EXPERTS, D, FF), (D // 9) ** -0.5, 0.25, ((0, 4), (2, 8)))
    up_proj = centred(keys[6], (EXPERTS, D, FF), (D // 9) ** -0.5, 0.25, ((0, 4), (2, 8)))
    down_proj = centred(keys[7], (EXPERTS, FF, D), FF ** -0.5, 0.125, ((0, 4), (1, 8)))
    out_proj = centred(keys[8], (RW, D), RW ** -0.5, 0.09375, ((0, 8),))
    query_rows = centred(keys[9], (SEQUENCE_TOKENS, RW), 1.0, 6.0, ((0, 4), (1, 8)))
    key_rows = centred(keys[10], (SEQUENCE_TOKENS, RW), 1.0, 6.0, ((0, 4), (1, 8)))
    value_rows = centred(keys[11], (SEQUENCE_TOKENS, RW), 1.0, 6.0, ((0, 4), (1, 8)))
    retention_out = centred(keys[12], (SEQUENCE_TOKENS, RW), 1.0, 6.0, ((0, 4), (1, 8)))
    log_decay = draw_log_decay(jax.random.fold_in(keys[15], 71), 0)
    entry_state = centred(keys[14], (SEGS, RETENTION_HEADS, DK, DK), 4.0, 24.0, ((0, 4), (1, 8)), jnp.float32)
    return dict(residual_mid=residual_mid, out_grad=out_grad, norm_gain=norm_gain, expert_ids=expert_ids, expert_weights=expert_weights, gate_proj=gate_proj, up_proj=up_proj, down_proj=down_proj, out_proj=out_proj, query_rows=query_rows, key_rows=key_rows, value_rows=value_rows, retention_out=retention_out, log_decay=log_decay, entry_state=entry_state)


CLAMP_LIMIT = 7.0
GATE_ALPHA = 1.702
NORM_EPSILON = 1e-05

def activate(gate_pre, up_pre):
    gate_clamped = jnp.minimum(gate_pre, CLAMP_LIMIT)
    up_clamped = jnp.clip(up_pre, -CLAMP_LIMIT, CLAMP_LIMIT)
    return (up_clamped + 1.0) * gate_clamped * jax.nn.sigmoid(GATE_ALPHA * gate_clamped)

def reference(residual_mid, out_grad, norm_gain, expert_ids, expert_weights, gate_proj, up_proj, down_proj, out_proj, query_rows, key_rows, value_rows, retention_out, log_decay, entry_state):
    top_count = expert_ids.shape[1]
    width = residual_mid.shape[1]
    pair_count = SEQUENCE_TOKENS * top_count
    mid_rows = residual_mid.astype(jnp.float32)
    inverse = lax.rsqrt(lax.optimization_barrier(jnp.mean(mid_rows * mid_rows, axis=1, keepdims=True)) + NORM_EPSILON)
    scaled = mid_rows * inverse
    normed = (scaled * norm_gain).astype(jnp.bfloat16)
    flat_ids = expert_ids.reshape(SEGS, TOK_DEV * top_count).astype(jnp.int32)
    chosen = (flat_ids[:, :, None] == jnp.arange(EXPERTS, dtype=jnp.int32)[None, None, :]).astype(jnp.int32)
    placed = lax.optimization_barrier(jnp.sum((jnp.cumsum(chosen, axis=1) - chosen) * chosen, axis=2)).astype(jnp.int32)
    segment = jnp.broadcast_to(jnp.arange(SEGS, dtype=jnp.int32)[:, None], flat_ids.shape)
    pair_index = jnp.arange(pair_count, dtype=jnp.int32).reshape(SEGS, TOK_DEV * top_count)
    slot_pair = jnp.full((EXPERTS, SEGS, CAP), pair_count, jnp.int32).at[flat_ids, segment, placed].set(pair_index)
    blank = jnp.zeros((1, width), jnp.bfloat16)
    token_table = jnp.concatenate([jnp.repeat(normed, top_count, axis=0), blank], axis=0)
    pair_grads = (expert_weights[:, :, None] * out_grad[:, None, :]).astype(jnp.bfloat16).reshape(pair_count, width)
    grad_table = jnp.concatenate([pair_grads, blank], axis=0)
    group_width = FF // N_TP

    def one_expert(operands):
        slot_rows, gate_weight, up_weight, down_weight = operands
        slot_index = slot_rows.reshape(-1)
        rows_in = token_table[slot_index]
        rows_grad = grad_table[slot_index]
        gate_pre = jnp.dot(rows_in, gate_weight, preferred_element_type=jnp.float32)
        up_pre = jnp.dot(rows_in, up_weight, preferred_element_type=jnp.float32)
        hidden, pullback = jax.vjp(activate, gate_pre, up_pre)
        down_part = jnp.dot(hidden.astype(jnp.bfloat16).T, rows_grad, preferred_element_type=jnp.float32).astype(jnp.bfloat16)
        hidden_grad = jnp.dot(rows_grad, down_weight.T, preferred_element_type=jnp.float32)
        gate_back, up_back = pullback(hidden_grad)
        gate_back = gate_back.astype(jnp.bfloat16)
        up_back = up_back.astype(jnp.bfloat16)
        gate_part = jnp.dot(rows_in.T, gate_back, preferred_element_type=jnp.float32).astype(jnp.bfloat16)
        up_part = jnp.dot(rows_in.T, up_back, preferred_element_type=jnp.float32).astype(jnp.bfloat16)
        row_total = rows_in.shape[0]
        parts = jnp.einsum('rjf,djf->jrd', gate_back.astype(jnp.float32).reshape(row_total, N_TP, group_width), gate_weight.astype(jnp.float32).reshape(width, N_TP, group_width))
        parts = parts + jnp.einsum('rjf,djf->jrd', up_back.astype(jnp.float32).reshape(row_total, N_TP, group_width), up_weight.astype(jnp.float32).reshape(width, N_TP, group_width))
        rounded = lax.optimization_barrier(parts.astype(jnp.bfloat16))
        summed = lax.optimization_barrier(jnp.sum(rounded.astype(jnp.float32), axis=0)).astype(jnp.bfloat16)
        return (gate_part, up_part, down_part, summed)
    gate_grad, up_grad, down_grad, returned = lax.map(one_expert, (slot_pair, gate_proj, up_proj, down_proj))
    picked = returned[flat_ids, segment * CAP + placed]
    mixed_grad = lax.optimization_barrier(jnp.sum(picked.reshape(SEQUENCE_TOKENS, top_count, width).astype(jnp.float32), axis=1))
    weighted = norm_gain * mixed_grad
    inner = lax.optimization_barrier(jnp.mean(scaled * weighted, axis=1, keepdims=True))
    resid_grad = (out_grad.astype(jnp.float32) + inverse * (weighted - scaled * inner)).astype(jnp.bfloat16)
    proj_grad = jnp.dot(resid_grad.T, retention_out, preferred_element_type=jnp.float32)
    head_grad = jnp.dot(resid_grad, out_proj.T, preferred_element_type=jnp.float32)
    heads = log_decay.shape[1]
    highest = lax.Precision.HIGHEST

    def split_heads(rows):
        return rows.astype(jnp.float32).reshape(SEGS, TOK_DEV, heads, -1).transpose(0, 2, 1, 3)
    queries = split_heads(query_rows)
    key_heads = split_heads(key_rows)
    value_heads = split_heads(value_rows)
    grad_heads = split_heads(head_grad)
    key_scale = queries.shape[3] ** (-0.5)
    running = jnp.cumsum(log_decay.reshape(SEGS, TOK_DEV, heads), axis=1).transpose(0, 2, 1)
    from_start = jnp.exp(running)
    to_end = jnp.exp(running[:, :, -1:] - running)
    token_position = jnp.arange(TOK_DEV, dtype=jnp.int32)
    causal = (token_position[:, None] >= token_position[None, :])[None, None]
    spread = jnp.where(causal, running[:, :, :, None] - running[:, :, None, :], 0.0)
    weights = jnp.where(causal, jnp.exp(spread), 0.0)
    local_state = jnp.einsum('ght,ghtk,ghte->ghke', from_start, queries, grad_heads, precision=highest)
    carry_rate = from_start[:, :, -1]

    def backward_step(carried, inputs):
        rate_now, local_now = inputs
        return (local_now + rate_now[:, None, None] * carried, carried)
    later_state = lax.scan(backward_step, jnp.zeros(local_state.shape[1:], jnp.float32), (carry_rate, local_state), reverse=True)[1]
    grad_scores = jnp.einsum('ghte,ghse->ghts', grad_heads, value_heads, precision=highest) * weights
    key_scores = jnp.einsum('ghtk,ghsk->ghts', queries, key_heads, precision=highest) * weights
    query_grad = key_scale * (jnp.einsum('ghts,ghsk->ghtk', grad_scores, key_heads, precision=highest) + from_start[..., None] * jnp.einsum('ghte,ghke->ghtk', grad_heads, entry_state, precision=highest))
    key_grad = key_scale * (jnp.einsum('ghts,ghtk->ghsk', grad_scores, queries, precision=highest) + to_end[..., None] * jnp.einsum('ghse,ghke->ghsk', value_heads, later_state, precision=highest))
    value_grad = key_scale * (jnp.einsum('ghts,ghte->ghse', key_scores, grad_heads, precision=highest) + to_end[..., None] * jnp.einsum('ghsk,ghke->ghse', key_heads, later_state, precision=highest))

    def merge_heads(heads_rows):
        return heads_rows.transpose(0, 2, 1, 3).reshape(SEQUENCE_TOKENS, -1).astype(jnp.bfloat16)
    return (gate_grad, up_grad, down_grad, proj_grad, merge_heads(query_grad), merge_heads(key_grad), merge_heads(value_grad))
```

```python
import functools

import jax
import jax.numpy as jnp
from jax import lax
from jax.experimental import pallas as pl
from jax.experimental.pallas import tpu as pltpu
from jax.sharding import Mesh, PartitionSpec as P

CLAMP_LIMIT = 7.0
GATE_ALPHA = 1.702
NORM_EPSILON = 1e-05
CORES = 2
SWAP = [(0, 1), (1, 0)]


def activate(gate_pre, up_pre):
    gate_clamped = jnp.minimum(gate_pre, CLAMP_LIMIT)
    up_clamped = jnp.clip(up_pre, -CLAMP_LIMIT, CLAMP_LIMIT)
    return (up_clamped + 1.0) * gate_clamped * jax.nn.sigmoid(GATE_ALPHA * gate_clamped)


def contract_rows(left, right):
    return lax.dot_general(
        left, right, (((0,), (0,)), ((), ())), preferred_element_type=jnp.float32
    )


def contract_cols(left, right):
    return lax.dot_general(
        left, right, (((1,), (1,)), ((), ())), preferred_element_type=jnp.float32
    )


def dots(spec, left, right):
    return jnp.einsum(
        spec,
        left.astype(jnp.bfloat16),
        right.astype(jnp.bfloat16),
        preferred_element_type=jnp.float32,
    )


def local_general(
    residual_mid,
    out_grad,
    norm_gain,
    expert_ids,
    expert_weights,
    gate_proj,
    up_proj,
    down_proj,
    out_proj,
    query_rows,
    key_rows,
    value_rows,
    retention_out,
    log_decay,
    entry_state,
):
    token_count, width = residual_mid.shape
    segs = lax.axis_size("sp")
    depth = lax.axis_size("z")
    seg = lax.axis_index("sp")
    core = lax.axis_index("core")
    half = token_count // CORES
    share = half // depth

    def rows_of(array, start, count):
        return lax.dynamic_slice_in_dim(array, start, count, axis=0)

    def normalize(rows):
        wide = rows.astype(jnp.float32)
        inverse = lax.rsqrt(jnp.mean(wide * wide, axis=1, keepdims=True) + NORM_EPSILON)
        return wide * inverse, inverse

    grad_own = lax.all_gather(rows_of(out_grad, core * half, half), "sp").reshape(-1, width)
    normed_half = (normalize(rows_of(residual_mid, core * half, half))[0] * norm_gain).astype(
        jnp.bfloat16
    )
    normed_own = lax.all_gather(normed_half, "sp").reshape(-1, width)
    grad_other = lax.ppermute(grad_own, "core", SWAP)
    normed_other = lax.ppermute(normed_own, "core", SWAP)

    experts = jnp.arange(segs, dtype=jnp.int32)
    route = jnp.sum(
        jnp.where(expert_ids.T[None] == experts[:, None, None], expert_weights.T[None], 0.0), axis=1
    )
    heads_here = log_decay.shape[1]
    small = jnp.concatenate([route.reshape(-1), jnp.sum(log_decay, axis=0)])
    smalls = lax.all_gather(small, "sp")
    routes = smalls[:, : segs * token_count].reshape(segs, segs, token_count)
    seg_decay = smalls[:, segs * token_count :]
    here = lax.dynamic_index_in_dim(routes, seg, axis=1, keepdims=False)
    here = here.reshape(segs, CORES, half)
    weight_own = lax.dynamic_index_in_dim(here, core, axis=1, keepdims=False).reshape(-1, 1)
    weight_other = lax.dynamic_index_in_dim(here, 1 - core, axis=1, keepdims=False).reshape(-1, 1)

    gate_weight = gate_proj[0]
    up_weight = up_proj[0]
    down_weight = down_proj[0]

    def expert(rows_in, rows_out, weight):
        rows_grad = (weight * rows_out.astype(jnp.float32)).astype(jnp.bfloat16)
        gate_pre = jnp.dot(rows_in, gate_weight, preferred_element_type=jnp.float32)
        up_pre = jnp.dot(rows_in, up_weight, preferred_element_type=jnp.float32)
        hidden, pullback = jax.vjp(activate, gate_pre, up_pre)
        gate_back, up_back = pullback(contract_cols(rows_grad, down_weight))
        gate_back = gate_back.astype(jnp.bfloat16)
        up_back = up_back.astype(jnp.bfloat16)
        part = contract_cols(gate_back, gate_weight) + contract_cols(up_back, up_weight)
        return part, rows_grad, hidden.astype(jnp.bfloat16), gate_back, up_back

    part_own, cot_own, hidden_own, gate_back_own, up_back_own = expert(
        normed_own, grad_own, weight_own
    )
    part_other, cot_other, hidden_other, gate_back_other, up_back_other = expert(
        normed_other, grad_other, weight_other
    )
    part_got = lax.ppermute(part_other.astype(jnp.bfloat16), "core", SWAP)
    part_pair = (part_own + part_got.astype(jnp.float32)).astype(jnp.bfloat16)
    part_seg = lax.psum_scatter(
        part_pair.reshape(segs, half, width), "sp", scatter_dimension=0, tiled=False
    )
    mixed_grad = lax.psum_scatter(
        part_seg.reshape(depth, share, width), "z", scatter_dimension=0, tiled=False
    ).astype(jnp.float32)

    down_grad = (contract_rows(hidden_own, cot_own) + contract_rows(hidden_other, cot_other)).astype(
        jnp.bfloat16
    )[None]
    gate_grad = (
        contract_rows(normed_own, gate_back_own) + contract_rows(normed_other, gate_back_other)
    ).astype(jnp.bfloat16)[None]
    up_grad = (
        contract_rows(normed_own, up_back_own) + contract_rows(normed_other, up_back_other)
    ).astype(jnp.bfloat16)[None]

    start = core * half + lax.axis_index("z") * share
    scaled, inverse = normalize(rows_of(residual_mid, start, share))
    weighted = norm_gain * mixed_grad
    inner = jnp.mean(scaled * weighted, axis=1, keepdims=True)
    resid_part = (
        rows_of(out_grad, start, share).astype(jnp.float32)
        + inverse * (weighted - scaled * inner)
    ).astype(jnp.bfloat16)
    resid_grad = lax.all_gather(resid_part, ("core", "z"), axis=0, tiled=False).reshape(
        token_count, width
    )
    columns = lax.all_to_all(
        resid_part.reshape(share, segs, width // segs).transpose(1, 0, 2),
        "sp",
        split_axis=0,
        concat_axis=0,
        tiled=True,
    )
    columns = lax.all_gather(columns, ("core", "z"), axis=0, tiled=False).reshape(
        segs * token_count, -1
    )
    outs = lax.all_gather(retention_out, "sp")
    outs = outs.reshape(segs, CORES * depth, share, -1).transpose(1, 0, 2, 3)
    outs = outs.reshape(segs * token_count, -1)
    proj_grad = contract_rows(columns, outs)

    head_grad = contract_cols(resid_grad, out_proj).astype(jnp.bfloat16)

    def split_heads(rows):
        return rows.reshape(token_count, heads_here, -1).transpose(1, 0, 2)

    queries = split_heads(query_rows)
    key_heads = split_heads(key_rows)
    value_heads = split_heads(value_rows)
    grad_heads = split_heads(head_grad)
    key_scale = queries.shape[2] ** (-0.5)
    running = jnp.cumsum(log_decay, axis=0).T
    from_start = jnp.exp(running)
    to_end = jnp.exp(running[:, -1:] - running)
    position = jnp.arange(token_count, dtype=jnp.int32)
    causal = (position[:, None] >= position[None, :])[None]
    spread = jnp.where(causal, running[:, :, None] - running[:, None, :], 0.0)
    weights = jnp.where(causal, jnp.exp(spread), 0.0)
    local_state = dots("htk,hte->hke", from_start[:, :, None] * queries, grad_heads)
    states = lax.all_gather(local_state.astype(jnp.bfloat16), "sp")
    order = jnp.arange(segs, dtype=jnp.int32)
    between = (order[None, :] > seg) & (order[None, :] < order[:, None])
    passed = jnp.exp(jnp.sum(jnp.where(between[:, :, None], seg_decay[None], 0.0), axis=1))
    passed = jnp.where(order[:, None] > seg, passed, 0.0)
    later_state = jnp.sum(passed[:, :, None, None] * states.astype(jnp.float32), axis=0)
    entry = entry_state[0]
    grad_scores = dots("hte,hse->hts", grad_heads, value_heads) * weights
    key_scores = dots("htk,hsk->hts", queries, key_heads) * weights
    query_grad = key_scale * (
        dots("hts,hsk->htk", grad_scores, key_heads)
        + from_start[:, :, None] * dots("hte,hke->htk", grad_heads, entry)
    )
    key_grad = key_scale * (
        dots("hts,htk->hsk", grad_scores, queries)
        + to_end[:, :, None] * dots("hse,hke->hsk", value_heads, later_state)
    )
    value_grad = key_scale * (
        dots("hts,hte->hse", key_scores, grad_heads)
        + to_end[:, :, None] * dots("hsk,hke->hse", key_heads, later_state)
    )

    def merge_heads(heads_rows):
        return heads_rows.transpose(1, 0, 2).reshape(token_count, -1).astype(jnp.bfloat16)

    return (
        gate_grad,
        up_grad,
        down_grad,
        proj_grad,
        merge_heads(query_grad),
        merge_heads(key_grad),
        merge_heads(value_grad),
    )


ROWS = 16
MESH_ID = pl.DeviceIdType.MESH


def square_kernel(
    raw_r_hbm,
    raw_o_hbm,
    route_ref,
    gain_ref,
    wg_hbm,
    wu_hbm,
    wd_hbm,
    op_hbm,
    outs_hbm,
    fq_hbm,
    ends_ref,
    gate_out,
    up_out,
    down_out,
    col_out,
    hg_out,
    outs_out,
    fq_out,
    ends_out,
    raw_r,
    raw_o,
    rin,
    og,
    stg,
    wg,
    wu,
    wd,
    op,
    part,
    pin,
    hid,
    back,
    rx,
    ry,
    rz1,
    sd,
    rd,
    rz2,
    wz,
    inv,
    msend,
    mz,
    rg,
    col,
    hga,
    outs_all,
    fq_all,
    ends_all,
    gout,
    uout,
    dout,
    send_sems,
    recv_sems,
    load_sems,
    store_sems,
):
    segs, count, width = rin.shape
    half = count // CORES
    depth = segs
    quarter = width // depth
    feats = wg.shape[1]
    g = lax.axis_index("sp")
    z = lax.axis_index("z")
    c = lax.axis_index("core")
    gy_, gx_ = g // 2, g % 2
    gx = gy_ * 2 + (1 - gx_)
    gy = (1 - gy_) * 2 + gx_
    gd = (1 - gy_) * 2 + (1 - gx_)
    ups = [(z + i) % depth for i in range(1, depth)]
    downs = [(z + depth - i) % depth for i in range(1, depth)]
    mine = pl.ds(pl.multiple_of(c * half, ROWS), half)
    theirs = pl.ds(pl.multiple_of((1 - c) * half, ROWS), half)

    def span(index):
        return pl.ds(pl.multiple_of(index * quarter, 128), quarter)

    def dev(sp, zz, cc):
        return {"sp": sp, "z": zz, "core": cc}

    sends = []
    used = [0]

    def remote(src, dst, target):
        k = used[0]
        used[0] += 1
        copy = pltpu.make_async_remote_copy(
            src_ref=src,
            dst_ref=dst,
            send_sem=send_sems.at[k],
            recv_sem=recv_sems.at[k],
            device_id=target,
            device_id_type=MESH_ID,
        )
        sends.append(copy)
        return copy

    def put(src, dst, target):
        copy = remote(src, dst, target)
        copy.start()
        return copy

    loads = []

    def load(src, dst):
        copy = pltpu.make_async_copy(src, dst, load_sems.at[len(loads)])
        copy.start()
        loads.append(copy)
        return copy

    stores = []

    def store(src, dst):
        copy = pltpu.make_async_copy(src, dst, store_sems.at[len(stores)])
        copy.start()
        stores.append(copy)

    load_o = load(raw_o_hbm, raw_o)
    load_r = load(raw_r_hbm, raw_r)
    load_w = [load(wg_hbm, wg), load(wu_hbm, wu), load(wd_hbm, wd)]
    load_op = load(op_hbm, op)
    load_outs = load(outs_hbm, outs_all.at[g])
    load_fq = load(fq_hbm, fq_all.at[g])

    X, Y, Z = dev(gx, z, c), dev(gy, z, c), dev(gd, z, c)
    across = dev(g, z, 1 - c)
    along = [dev(g, zz, c) for zz in ups]
    barrier = pltpu.get_barrier_semaphore()
    for target in [X, Y, Z, across] + along:
        pl.semaphore_signal(barrier, inc=1, device_id=target, device_id_type=MESH_ID)

    lanes = lax.broadcasted_iota(jnp.int32, (ROWS, 128), 1)

    def weigh(base, rows, expert, write):
        def step(i, carry):
            r = pl.ds(pl.multiple_of(base + i * ROWS, ROWS), ROWS)
            w = jnp.sum(jnp.where(lanes == expert, route_ref[r, :], 0.0), axis=1, keepdims=True)
            write(i, r, (w * raw_o[r, :].astype(jnp.float32)).astype(jnp.bfloat16))
            return carry

        lax.fori_loop(0, rows // ROWS, step, 0)

    def stage(index):
        def write(i, r, value):
            stg[index, pl.ds(pl.multiple_of(i * ROWS, ROWS), ROWS), :] = value

        return write

    def own_write(i, r, value):
        og[g, r, :] = value

    def normalize(base, rows):
        def step(i, carry):
            r = pl.ds(pl.multiple_of(base + i * ROWS, ROWS), ROWS)
            wide = raw_r[r, :].astype(jnp.float32)
            inverse = lax.rsqrt(jnp.mean(wide * wide, axis=1, keepdims=True) + NORM_EPSILON)
            inv[r, :] = jnp.broadcast_to(inverse, (ROWS, 128))
            rin[g, r, :] = (wide * inverse * gain_ref[...]).astype(jnp.bfloat16)
            return carry

        lax.fori_loop(0, rows // ROWS, step, 0)

    load_o.wait()
    weigh(c * half, half, gd, stage(2))
    pl.semaphore_wait(barrier, 4 + len(along))
    d_o = put(stg.at[2, :, span(z)], og.at[g, mine, span(z)], Z)
    load_r.wait()
    normalize(c * half, half)
    d_n = put(rin.at[g, mine, span(z)], rin.at[g, mine, span(z)], Z)
    x_n = put(rin.at[g, mine, :], rin.at[g, mine, :], X)
    y_n = put(rin.at[g, mine, :], rin.at[g, mine, :], Y)
    weigh(c * half, half, gx, stage(0))
    x_o = put(stg.at[0], og.at[g, mine, :], X)
    weigh(c * half, half, gy, stage(1))
    y_o = put(stg.at[1], og.at[g, mine, :], Y)
    normalize((1 - c) * half, half)
    weigh(0, count, g, own_write)

    def spread(buf):
        block = buf.at[gd, mine, span(z)]
        return [put(block, block, t) for t in along] + [put(block, block, across)]

    d_o.wait_recv()
    o_spread = spread(og)
    d_n.wait_recv()
    n_spread = spread(rin)

    for copy in load_w:
        copy.wait()

    def expert(s):
        gate_pre = jnp.dot(rin[s], wg[...], preferred_element_type=jnp.float32)
        up_pre = jnp.dot(rin[s], wu[...], preferred_element_type=jnp.float32)
        hidden, pullback = jax.vjp(activate, gate_pre, up_pre)
        gate_back, up_back = pullback(contract_cols(og[s], wd[...]))
        gate_back = gate_back.astype(jnp.bfloat16)
        up_back = up_back.astype(jnp.bfloat16)
        hid[s] = hidden.astype(jnp.bfloat16)
        back[s, :, :feats] = gate_back
        back[s, :, feats:] = up_back

        def step(n, carry):
            rows = pl.ds(pl.multiple_of(n * quarter, 128), quarter)
            piece = contract_cols(back[s, :, :feats], wg[rows, :]) + contract_cols(
                back[s, :, feats:], wu[rows, :]
            )
            part[s, :, rows] = piece.astype(jnp.bfloat16)
            return carry

        lax.fori_loop(0, depth, step, 0)
        return put(part.at[s, theirs, :], pin.at[s], across)

    swap_own = expert(g)

    x_n.wait_recv()
    f = [put(rin.at[gx, mine, :], rin.at[gx, mine, :], across)]
    y_n.wait_recv()
    f.append(put(rin.at[gy, mine, :], rin.at[gy, mine, :], across))
    for i in range(depth - 1):
        for buf, group in ((og, o_spread), (rin, n_spread)):
            group[i].wait_recv()
            block = buf.at[gd, mine, span(downs[i])]
            f.append(put(block, block, across))
    x_o.wait_recv()
    f.append(put(og.at[gx, mine, :], og.at[gx, mine, :], across))
    y_o.wait_recv()
    f.append(put(og.at[gy, mine, :], og.at[gy, mine, :], across))
    o_spread[-1].wait_recv()
    n_spread[-1].wait_recv()
    for copy in f:
        copy.wait_recv()

    def pair(s, swap, extra=()):
        swap.wait_recv()

        def step(i, carry):
            r = pl.ds(pl.multiple_of(c * half + i * ROWS, ROWS), ROWS)
            q = pl.ds(pl.multiple_of(i * ROWS, ROWS), ROWS)
            total = part[s, r, :].astype(jnp.float32) + pin[s, q, :].astype(jnp.float32)
            for ref in extra:
                total = total + ref[q, :].astype(jnp.float32)
            part[s, r, :] = total.astype(jnp.bfloat16)
            return carry

        lax.fori_loop(0, half // ROWS, step, 0)

    swap_d = expert(gd)
    swap_x = expert(gx)
    pair(gd, swap_d)
    d_z = [put(part.at[gd, mine, span(ups[i])], rz1.at[i], along[i]) for i in range(depth - 1)]
    swap_y = expert(gy)
    pair(gx, swap_x)
    x_p = put(part.at[gx, mine, :], rx, X)
    pair(gy, swap_y)
    y_p = put(part.at[gy, mine, :], ry, Y)

    def weight_step(n, carry):
        cols = pl.ds(pl.multiple_of(n * 512, 128), 512)
        block = contract_rows(rin[:, :, cols].reshape(segs * count, 512), back[...].reshape(segs * count, 2 * feats))
        gout[cols, :] = block[:, :feats].astype(jnp.bfloat16)
        uout[cols, :] = block[:, feats:].astype(jnp.bfloat16)
        return carry

    lax.fori_loop(0, width // 512, weight_step, 0)
    store(gout, gate_out)
    store(uout, up_out)

    def z_sum(own, landed, write, more=None):
        for copy in landed[0]:
            copy.wait_recv()

        def step(i, carry):
            q = pl.ds(pl.multiple_of(i * ROWS, ROWS), ROWS)
            r = pl.ds(pl.multiple_of(c * half + i * ROWS, ROWS), ROWS)
            total = part[own, r, span(z)].astype(jnp.float32)
            for k in range(depth - 1):
                total = total + landed[1][k, q, :].astype(jnp.float32)
            if more is not None:
                total = total + more[q, :].astype(jnp.float32)
            write(q, r, total)
            return carry

        lax.fori_loop(0, half // ROWS, step, 0)

    def write_sd(q, r, total):
        sd[q, :] = total.astype(jnp.bfloat16)

    z_sum(gd, (d_z, rz1), write_sd)
    d_p = put(sd, rd, Z)

    load_outs.wait()
    load_fq.wait()
    extras = []
    for target in (X, Y, Z):
        extras.append(put(fq_all.at[g], fq_all.at[g], target))
        extras.append(put(ends_ref, ends_all.at[g], target))
        extras.append(put(outs_all.at[g], outs_all.at[g], target))
    ends_all[g] = ends_ref[...]

    x_p.wait_recv()
    y_p.wait_recv()
    pair(g, swap_own, (rx, ry))
    own_z = [put(part.at[g, mine, span(ups[i])], rz2.at[i], along[i]) for i in range(depth - 1)]

    def down_step(n, carry):
        cols = pl.ds(pl.multiple_of(n * 512, 128), 512)
        block = contract_rows(
            hid[...].reshape(segs * count, feats), og[:, :, cols].reshape(segs * count, 512)
        )
        dout[:, cols] = block.astype(jnp.bfloat16)
        return carry

    lax.fori_loop(0, width // 512, down_step, 0)
    store(dout, down_out)

    d_p.wait_recv()

    def write_m(q, r, total):
        weighted = gain_ref[:, span(z)] * total
        scaled = raw_r[r, span(z)].astype(jnp.float32) * inv[r, 0:1]
        inner = jnp.sum(scaled * weighted, axis=1, keepdims=True)
        msend[q, :] = jnp.broadcast_to(inner, (ROWS, 128))
        wz[q, :] = weighted

    z_sum(g, (own_z, rz2), write_m, rd)
    m_z = [put(msend, mz.at[i], along[i]) for i in range(depth - 1)]
    for copy in m_z:
        copy.wait_recv()

    def resid_step(i, carry):
        q = pl.ds(pl.multiple_of(i * ROWS, ROWS), ROWS)
        r = pl.ds(pl.multiple_of(c * half + i * ROWS, ROWS), ROWS)
        inverse = inv[r, 0:1]
        scaled = raw_r[r, span(z)].astype(jnp.float32) * inverse
        inner = msend[q, 0:1]
        for k in range(depth - 1):
            inner = inner + mz[k, q, 0:1]
        inner = inner / width
        grad = raw_o[r, span(z)].astype(jnp.float32) + inverse * (wz[q, :] - scaled * inner)
        rg[r, span(z)] = grad.astype(jnp.bfloat16)
        return carry

    lax.fori_loop(0, half // ROWS, resid_step, 0)
    block = rg.at[mine, span(z)]
    g_z = [put(block, block, t) for t in along]
    g_f = [put(block, block, across)]
    col_copies = [
        (t, remote(rg.at[mine, span(t)], col.at[g, mine, :], target))
        for t, target in ((gx, X), (gy, Y), (gd, Z))
    ]

    def send_columns(q):
        for t, copy in col_copies:

            @pl.when(q == t)
            def _():
                copy.start()

    send_columns(z)
    for i in range(depth - 1):
        g_z[i].wait_recv()
        block = rg.at[mine, span(downs[i])]
        g_f.append(put(block, block, across))
        send_columns(downs[i])
    for copy in g_f:
        copy.wait_recv()
    load_op.wait()
    hga[g] = contract_cols(rg[...], op[...]).astype(jnp.bfloat16)
    heads = [put(hga.at[g], hga.at[g], t) for t in (X, Y, Z)]
    col[g] = rg[:, span(g)]
    col_f = []
    for (t, copy) in col_copies:
        copy.wait_recv()
        block = col.at[t, mine, :]
        col_f.append(put(block, block, across))
    for copy in extras:
        copy.wait_recv()
    store(outs_all, outs_out)
    store(fq_all, fq_out)
    store(ends_all, ends_out)
    for copy in col_f:
        copy.wait_recv()
    store(col, col_out)
    for copy in heads:
        copy.wait_recv()
    store(hga, hg_out)
    for copy in sends:
        copy.wait_send()
    for copy in stores:
        copy.wait()


def square_call(segs, raw_r, raw_o, route, gain, wg, wu, wd, op, outs, fq, ends):
    count, width = raw_r.shape
    feats, heads = wg.shape[1], outs.shape[1]
    half, quarter = count // CORES, width // segs
    bf16, f32 = jnp.bfloat16, jnp.float32
    any_spec = pl.BlockSpec(memory_space=pl.ANY)
    vmem_spec = pl.BlockSpec(memory_space=pltpu.VMEM)
    shape = jax.ShapeDtypeStruct
    flops = 2 * segs * count * width * feats * 8
    return pl.pallas_call(
        square_kernel,
        out_shape=(
            shape((width, feats), bf16),
            shape((width, feats), bf16),
            shape((feats, width), bf16),
            shape((segs, count, quarter), bf16),
            shape((segs, count, heads), bf16),
            shape((segs, count, heads), bf16),
            shape((segs, count, heads), bf16),
            shape((segs, 8, 128), f32),
        ),
        in_specs=[any_spec, any_spec, vmem_spec, vmem_spec]
        + [any_spec] * 6
        + [vmem_spec],
        out_specs=(any_spec,) * 8,
        scratch_shapes=[
            pltpu.VMEM((count, width), bf16),
            pltpu.VMEM((count, width), bf16),
            pltpu.VMEM((segs, count, width), bf16),
            pltpu.VMEM((segs, count, width), bf16),
            pltpu.VMEM((3, half, width), bf16),
            pltpu.VMEM((width, feats), bf16),
            pltpu.VMEM((width, feats), bf16),
            pltpu.VMEM((feats, width), bf16),
            pltpu.VMEM((heads, width), bf16),
            pltpu.VMEM((segs, count, width), bf16),
            pltpu.VMEM((segs, half, width), bf16),
            pltpu.VMEM((segs, count, feats), bf16),
            pltpu.VMEM((segs, count, 2 * feats), bf16),
            pltpu.VMEM((half, width), bf16),
            pltpu.VMEM((half, width), bf16),
            pltpu.VMEM((segs - 1, half, quarter), bf16),
            pltpu.VMEM((half, quarter), bf16),
            pltpu.VMEM((half, quarter), bf16),
            pltpu.VMEM((segs - 1, half, quarter), bf16),
            pltpu.VMEM((half, quarter), f32),
            pltpu.VMEM((count, 128), f32),
            pltpu.VMEM((half, 128), f32),
            pltpu.VMEM((segs - 1, half, 128), f32),
            pltpu.VMEM((count, width), bf16),
            pltpu.VMEM((segs, count, quarter), bf16),
            pltpu.VMEM((segs, count, heads), bf16),
            pltpu.VMEM((segs, count, heads), bf16),
            pltpu.VMEM((segs, count, heads), bf16),
            pltpu.VMEM((segs, 8, 128), f32),
            pltpu.VMEM((width, feats), bf16),
            pltpu.VMEM((width, feats), bf16),
            pltpu.VMEM((feats, width), bf16),
            pltpu.SemaphoreType.DMA((72,)),
            pltpu.SemaphoreType.DMA((72,)),
            pltpu.SemaphoreType.DMA((8,)),
            pltpu.SemaphoreType.DMA((8,)),
        ],
        compiler_params=pltpu.CompilerParams(
            collective_id=0, has_side_effects=True, vmem_limit_bytes=66 * 1000 * 1000
        ),
        cost_estimate=pl.CostEstimate(flops=flops, bytes_accessed=40000000, transcendentals=0),
    )(raw_r, raw_o, route, gain, wg, wu, wd, op, outs, fq, ends)


def local_square(
    residual_mid,
    out_grad,
    norm_gain,
    expert_ids,
    expert_weights,
    gate_proj,
    up_proj,
    down_proj,
    out_proj,
    query_rows,
    key_rows,
    value_rows,
    retention_out,
    log_decay,
    entry_state,
):
    token_count, width = residual_mid.shape
    segs = lax.axis_size("sp")
    seg = lax.axis_index("sp")
    heads_here = log_decay.shape[1]
    experts = jnp.arange(128, dtype=jnp.int32)
    route = jnp.sum(
        jnp.where(
            expert_ids[:, :, None] == experts[None, None, :], expert_weights[:, :, None], 0.0
        ),
        axis=1,
    )

    def split_heads(rows):
        return rows.reshape(token_count, heads_here, -1).transpose(1, 0, 2)

    running = jnp.cumsum(log_decay, axis=0).T
    from_start = jnp.exp(running)
    head_width = query_rows.shape[1] // heads_here
    fq = (
        jnp.repeat(from_start.T, head_width, axis=1) * query_rows.astype(jnp.float32)
    ).astype(jnp.bfloat16)
    ends = jnp.zeros((8, 128), jnp.float32).at[:, :heads_here].set(running[:, -1][None, :])
    gate_grad, up_grad, down_grad, columns, grads, outs, fqs, ends_all = square_call(
        segs,
        residual_mid,
        out_grad,
        route,
        norm_gain.reshape(1, width),
        gate_proj[0],
        up_proj[0],
        down_proj[0],
        out_proj,
        retention_out,
        fq,
        ends,
    )
    proj_grad = contract_rows(
        columns.reshape(segs * token_count, -1), outs.reshape(segs * token_count, -1)
    )
    seg_decay = ends_all[:, 0, :heads_here]
    head_grad = lax.dynamic_index_in_dim(grads, seg, axis=0, keepdims=False)
    queries = split_heads(query_rows)
    key_heads = split_heads(key_rows)
    value_heads = split_heads(value_rows)
    grad_heads = split_heads(head_grad)
    key_scale = queries.shape[2] ** (-0.5)
    to_end = jnp.exp(running[:, -1:] - running)
    position = jnp.arange(token_count, dtype=jnp.int32)
    causal = (position[:, None] >= position[None, :])[None]
    spread = jnp.where(causal, running[:, :, None] - running[:, None, :], 0.0)
    weights = jnp.where(causal, jnp.exp(spread), 0.0)
    states = dots(
        "gthk,gthe->ghke",
        fqs.reshape(segs, token_count, heads_here, head_width),
        grads.reshape(segs, token_count, heads_here, head_width),
    )
    order = jnp.arange(segs, dtype=jnp.int32)
    between = (order[None, :] > seg) & (order[None, :] < order[:, None])
    passed = jnp.exp(jnp.sum(jnp.where(between[:, :, None], seg_decay[None], 0.0), axis=1))
    passed = jnp.where(order[:, None] > seg, passed, 0.0)
    later_state = jnp.sum(passed[:, :, None, None] * states, axis=0)
    entry = entry_state[0]
    grad_scores = dots("hte,hse->hts", grad_heads, value_heads) * weights
    key_scores = dots("htk,hsk->hts", queries, key_heads) * weights
    query_grad = key_scale * (
        dots("hts,hsk->htk", grad_scores, key_heads)
        + from_start[:, :, None] * dots("hte,hke->htk", grad_heads, entry)
    )
    key_grad = key_scale * (
        dots("hts,htk->hsk", grad_scores, queries)
        + to_end[:, :, None] * dots("hse,hke->hsk", value_heads, later_state)
    )
    value_grad = key_scale * (
        dots("hts,hte->hse", key_scores, grad_heads)
        + to_end[:, :, None] * dots("hsk,hke->hse", key_heads, later_state)
    )

    def merge_heads(heads_rows):
        return heads_rows.transpose(1, 0, 2).reshape(token_count, -1).astype(jnp.bfloat16)

    return (
        gate_grad[None],
        up_grad[None],
        down_grad[None],
        proj_grad,
        merge_heads(query_grad),
        merge_heads(key_grad),
        merge_heads(value_grad),
    )


def solution(mesh):
    segs, split = mesh.shape["sp"], mesh.shape["tp"]
    fine = Mesh(mesh.devices.reshape(segs, split // CORES, CORES), ("sp", "z", "core"))
    tp = ("z", "core")
    placed = (
        P("sp", None),
        P("sp", None),
        P(),
        P("sp", None),
        P("sp", None),
        P("sp", None, tp),
        P("sp", None, tp),
        P("sp", tp, None),
        P(tp, None),
        P("sp", tp),
        P("sp", tp),
        P("sp", tp),
        P("sp", tp),
        P("sp", tp),
        P("sp", tp, None, None),
    )
    fast = segs == 4 and split == segs * CORES
    return jax.shard_map(
        local_square if fast else local_general,
        mesh=fine,
        in_specs=placed,
        out_specs=(
            P("sp", None, tp),
            P("sp", None, tp),
            P("sp", tp, None),
            P("sp", tp),
            P("sp", tp),
            P("sp", tp),
            P("sp", tp),
        ),
        check_vma=False,
    )
```

```python
import jax
import jax.numpy as jnp
from jax import lax
from jax.experimental import pallas as pl
from jax.experimental.pallas import tpu as pltpu
from jax.sharding import Mesh, PartitionSpec as P

CLAMP_LIMIT = 7.0
GATE_ALPHA = 1.702
NORM_EPSILON = 1e-05
CORES = 2
SWAP = [(0, 1), (1, 0)]


def activate(gate_pre, up_pre):
    gate_clamped = jnp.minimum(gate_pre, CLAMP_LIMIT)
    up_clamped = jnp.clip(up_pre, -CLAMP_LIMIT, CLAMP_LIMIT)
    return (up_clamped + 1.0) * gate_clamped * jax.nn.sigmoid(GATE_ALPHA * gate_clamped)


def contract_rows(left, right):
    return lax.dot_general(
        left, right, (((0,), (0,)), ((), ())), preferred_element_type=jnp.float32
    )


def contract_cols(left, right):
    return lax.dot_general(
        left, right, (((1,), (1,)), ((), ())), preferred_element_type=jnp.float32
    )


def dots(spec, left, right):
    return jnp.einsum(
        spec,
        left.astype(jnp.bfloat16),
        right.astype(jnp.bfloat16),
        preferred_element_type=jnp.float32,
    )


def local_general(
    residual_mid,
    out_grad,
    norm_gain,
    expert_ids,
    expert_weights,
    gate_proj,
    up_proj,
    down_proj,
    out_proj,
    query_rows,
    key_rows,
    value_rows,
    retention_out,
    log_decay,
    entry_state,
):
    token_count, width = residual_mid.shape
    segs = lax.axis_size("sp")
    depth = lax.axis_size("z")
    seg = lax.axis_index("sp")
    core = lax.axis_index("core")
    half = token_count // CORES
    share = half // depth

    def rows_of(array, start, count):
        return lax.dynamic_slice_in_dim(array, start, count, axis=0)

    def normalize(rows):
        wide = rows.astype(jnp.float32)
        inverse = lax.rsqrt(jnp.mean(wide * wide, axis=1, keepdims=True) + NORM_EPSILON)
        return wide * inverse, inverse

    grad_own = lax.all_gather(rows_of(out_grad, core * half, half), "sp").reshape(-1, width)
    normed_half = (normalize(rows_of(residual_mid, core * half, half))[0] * norm_gain).astype(
        jnp.bfloat16
    )
    normed_own = lax.all_gather(normed_half, "sp").reshape(-1, width)
    grad_other = lax.ppermute(grad_own, "core", SWAP)
    normed_other = lax.ppermute(normed_own, "core", SWAP)

    experts = jnp.arange(segs, dtype=jnp.int32)
    route = jnp.sum(
        jnp.where(expert_ids.T[None] == experts[:, None, None], expert_weights.T[None], 0.0), axis=1
    )
    heads_here = log_decay.shape[1]
    small = jnp.concatenate([route.reshape(-1), jnp.sum(log_decay, axis=0)])
    smalls = lax.all_gather(small, "sp")
    routes = smalls[:, : segs * token_count].reshape(segs, segs, token_count)
    seg_decay = smalls[:, segs * token_count :]
    here = lax.dynamic_index_in_dim(routes, seg, axis=1, keepdims=False)
    here = here.reshape(segs, CORES, half)
    weight_own = lax.dynamic_index_in_dim(here, core, axis=1, keepdims=False).reshape(-1, 1)
    weight_other = lax.dynamic_index_in_dim(here, 1 - core, axis=1, keepdims=False).reshape(-1, 1)

    gate_weight = gate_proj[0]
    up_weight = up_proj[0]
    down_weight = down_proj[0]

    def expert(rows_in, rows_out, weight):
        rows_grad = (weight * rows_out.astype(jnp.float32)).astype(jnp.bfloat16)
        gate_pre = jnp.dot(rows_in, gate_weight, preferred_element_type=jnp.float32)
        up_pre = jnp.dot(rows_in, up_weight, preferred_element_type=jnp.float32)
        hidden, pullback = jax.vjp(activate, gate_pre, up_pre)
        gate_back, up_back = pullback(contract_cols(rows_grad, down_weight))
        gate_back = gate_back.astype(jnp.bfloat16)
        up_back = up_back.astype(jnp.bfloat16)
        part = contract_cols(gate_back, gate_weight) + contract_cols(up_back, up_weight)
        return part, rows_grad, hidden.astype(jnp.bfloat16), gate_back, up_back

    part_own, cot_own, hidden_own, gate_back_own, up_back_own = expert(
        normed_own, grad_own, weight_own
    )
    part_other, cot_other, hidden_other, gate_back_other, up_back_other = expert(
        normed_other, grad_other, weight_other
    )
    part_got = lax.ppermute(part_other.astype(jnp.bfloat16), "core", SWAP)
    part_pair = (part_own + part_got.astype(jnp.float32)).astype(jnp.bfloat16)
    part_seg = lax.psum_scatter(
        part_pair.reshape(segs, half, width), "sp", scatter_dimension=0, tiled=False
    )
    mixed_grad = lax.psum_scatter(
        part_seg.reshape(depth, share, width), "z", scatter_dimension=0, tiled=False
    ).astype(jnp.float32)

    down_grad = (contract_rows(hidden_own, cot_own) + contract_rows(hidden_other, cot_other)).astype(
        jnp.bfloat16
    )[None]
    gate_grad = (
        contract_rows(normed_own, gate_back_own) + contract_rows(normed_other, gate_back_other)
    ).astype(jnp.bfloat16)[None]
    up_grad = (
        contract_rows(normed_own, up_back_own) + contract_rows(normed_other, up_back_other)
    ).astype(jnp.bfloat16)[None]

    start = core * half + lax.axis_index("z") * share
    scaled, inverse = normalize(rows_of(residual_mid, start, share))
    weighted = norm_gain * mixed_grad
    inner = jnp.mean(scaled * weighted, axis=1, keepdims=True)
    resid_part = (
        rows_of(out_grad, start, share).astype(jnp.float32)
        + inverse * (weighted - scaled * inner)
    ).astype(jnp.bfloat16)
    resid_grad = lax.all_gather(resid_part, ("core", "z"), axis=0, tiled=False).reshape(
        token_count, width
    )
    columns = lax.all_to_all(
        resid_part.reshape(share, segs, width // segs).transpose(1, 0, 2),
        "sp",
        split_axis=0,
        concat_axis=0,
        tiled=True,
    )
    columns = lax.all_gather(columns, ("core", "z"), axis=0, tiled=False).reshape(
        segs * token_count, -1
    )
    outs = lax.all_gather(retention_out, "sp")
    outs = outs.reshape(segs, CORES * depth, share, -1).transpose(1, 0, 2, 3)
    outs = outs.reshape(segs * token_count, -1)
    proj_grad = contract_rows(columns, outs)

    head_grad = contract_cols(resid_grad, out_proj).astype(jnp.bfloat16)

    def split_heads(rows):
        return rows.reshape(token_count, heads_here, -1).transpose(1, 0, 2)

    queries = split_heads(query_rows)
    key_heads = split_heads(key_rows)
    value_heads = split_heads(value_rows)
    grad_heads = split_heads(head_grad)
    key_scale = queries.shape[2] ** (-0.5)
    running = jnp.cumsum(log_decay, axis=0).T
    from_start = jnp.exp(running)
    to_end = jnp.exp(running[:, -1:] - running)
    position = jnp.arange(token_count, dtype=jnp.int32)
    causal = (position[:, None] >= position[None, :])[None]
    spread = jnp.where(causal, running[:, :, None] - running[:, None, :], 0.0)
    weights = jnp.where(causal, jnp.exp(spread), 0.0)
    local_state = dots("htk,hte->hke", from_start[:, :, None] * queries, grad_heads)
    states = lax.all_gather(local_state.astype(jnp.bfloat16), "sp")
    order = jnp.arange(segs, dtype=jnp.int32)
    between = (order[None, :] > seg) & (order[None, :] < order[:, None])
    passed = jnp.exp(jnp.sum(jnp.where(between[:, :, None], seg_decay[None], 0.0), axis=1))
    passed = jnp.where(order[:, None] > seg, passed, 0.0)
    later_state = jnp.sum(passed[:, :, None, None] * states.astype(jnp.float32), axis=0)
    entry = entry_state[0]
    grad_scores = dots("hte,hse->hts", grad_heads, value_heads) * weights
    key_scores = dots("htk,hsk->hts", queries, key_heads) * weights
    query_grad = key_scale * (
        dots("hts,hsk->htk", grad_scores, key_heads)
        + from_start[:, :, None] * dots("hte,hke->htk", grad_heads, entry)
    )
    key_grad = key_scale * (
        dots("hts,htk->hsk", grad_scores, queries)
        + to_end[:, :, None] * dots("hse,hke->hsk", value_heads, later_state)
    )
    value_grad = key_scale * (
        dots("hts,hte->hse", key_scores, grad_heads)
        + to_end[:, :, None] * dots("hsk,hke->hse", key_heads, later_state)
    )

    def merge_heads(heads_rows):
        return heads_rows.transpose(1, 0, 2).reshape(token_count, -1).astype(jnp.bfloat16)

    return (
        gate_grad,
        up_grad,
        down_grad,
        proj_grad,
        merge_heads(query_grad),
        merge_heads(key_grad),
        merge_heads(value_grad),
    )


ROWS = 16
VMEM_LIMIT = 66 * 1000 * 1000
MESH_ID = pl.DeviceIdType.MESH


def square_kernel(
    raw_r_hbm,
    raw_o_hbm,
    ids_ref,
    scale_ref,
    decay_ref,
    gain_ref,
    wg_hbm,
    wu_hbm,
    wd_hbm,
    op_hbm,
    outs_hbm,
    query_hbm,
    gate_out,
    up_out,
    down_out,
    col_out,
    hg_out,
    outs_out,
    fq_out,
    ends_out,
    raw_r,
    raw_o,
    rin,
    og,
    stg,
    wg,
    wu,
    wd,
    op,
    part,
    pin,
    hid,
    back,
    pre,
    hgrad,
    query,
    rx,
    ry,
    rdd,
    rz1,
    sd,
    rd,
    rz2,
    inv,
    route,
    means,
    mrow,
    mland,
    msend,
    mz,
    rg,
    col,
    hga,
    outs_all,
    fq_all,
    ends_all,
    gout,
    uout,
    dout,
    send_sems,
    recv_sems,
    load_sems,
    store_sems,
):
    segs, count, width = rin.shape
    half = count // CORES
    depth = segs
    quarter = width // depth
    feats = wg.shape[1]
    g = lax.axis_index("sp")
    z = lax.axis_index("z")
    c = lax.axis_index("core")
    gy_, gx_ = g // 2, g % 2
    gx = gy_ * 2 + (1 - gx_)
    gy = (1 - gy_) * 2 + gx_
    gd = (1 - gy_) * 2 + (1 - gx_)
    ups = [(z + i) % depth for i in range(1, depth)]
    downs = [(z + depth - i) % depth for i in range(1, depth)]
    mine = pl.ds(pl.multiple_of(c * half, ROWS), half)
    theirs = pl.ds(pl.multiple_of((1 - c) * half, ROWS), half)

    def span(index):
        return pl.ds(pl.multiple_of(index * quarter, 128), quarter)

    def dev(sp, zz, cc):
        return {"sp": sp, "z": zz, "core": cc}

    sends = []
    used = [0]

    def remote(src, dst, target):
        k = used[0]
        used[0] += 1
        copy = pltpu.make_async_remote_copy(
            src_ref=src,
            dst_ref=dst,
            send_sem=send_sems.at[k],
            recv_sem=recv_sems.at[k],
            device_id=target,
            device_id_type=MESH_ID,
        )
        sends.append(copy)
        return copy

    def put(src, dst, target):
        copy = remote(src, dst, target)
        copy.start()
        return copy

    def line_put(block):
        return [put(block, block, target) for target in along]

    loads = []

    def load(src, dst):
        copy = pltpu.make_async_copy(src, dst, load_sems.at[len(loads)])
        copy.start()
        loads.append(copy)
        return copy

    stores = []

    def store(src, dst):
        copy = pltpu.make_async_copy(src, dst, store_sems.at[len(stores)])
        copy.start()
        stores.append(copy)

    load_r = load(raw_r_hbm, raw_r)
    load_o = load(raw_o_hbm, raw_o)
    load_w = [load(wg_hbm, wg), load(wu_hbm, wu), load(wd_hbm, wd)]
    load_op = load(op_hbm, op)
    load_outs = load(outs_hbm, outs_all.at[0])
    load_query = load(query_hbm, query)

    X, Y, Z = dev(gx, z, c), dev(gy, z, c), dev(gd, z, c)
    across = dev(g, z, 1 - c)
    along = [dev(g, zz, c) for zz in ups]
    barrier = pltpu.get_barrier_semaphore()
    for target in [X, Y, Z, across] + along:
        pl.semaphore_signal(barrier, inc=1, device_id=target, device_id_type=MESH_ID)

    kinds = (g, gd, gx, gy)
    which = lax.broadcasted_iota(jnp.int32, (8, count), 0)
    table = jnp.zeros((8, count), jnp.float32)
    for k, expert in enumerate(kinds):
        chosen = jnp.where(ids_ref[...] == expert, scale_ref[...], 0.0)
        table = jnp.where(which == k, jnp.sum(chosen, axis=0, keepdims=True), table)
    unit = lax.broadcasted_iota(jnp.int32, (8, 128), 0) == lax.broadcasted_iota(
        jnp.int32, (8, 128), 1
    )
    exact = dict(preferred_element_type=jnp.float32, precision=lax.Precision.HIGHEST)
    route[...] = lax.dot_general(
        table, unit.astype(jnp.float32), (((0,), (0,)), ((), ())), **exact
    )

    def weigh(base, rows, kind, write):
        def step(i, carry):
            r = pl.ds(pl.multiple_of(base + i * ROWS, ROWS), ROWS)
            w = route[r, kind : kind + 1]
            write(i, r, (w * raw_o[r, :].astype(jnp.float32)).astype(jnp.bfloat16))
            return carry

        lax.fori_loop(0, rows // ROWS, step, 0)

    def stage(index):
        def write(i, r, value):
            stg[index, pl.ds(pl.multiple_of(i * ROWS, ROWS), ROWS), :] = value

        return write

    def own_write(i, r, value):
        og[0, r, :] = value

    def normalize(base, rows):
        def step(i, carry):
            r = pl.ds(pl.multiple_of(base + i * ROWS, ROWS), ROWS)
            wide = raw_r[r, :].astype(jnp.float32)
            inverse = lax.rsqrt(jnp.mean(wide * wide, axis=1, keepdims=True) + NORM_EPSILON)
            inv[r, :] = jnp.broadcast_to(inverse, (ROWS, 128))
            rin[0, r, :] = (wide * inverse * gain_ref[...]).astype(jnp.bfloat16)
            return carry

        lax.fori_loop(0, rows // ROWS, step, 0)

    load_r.wait()
    normalize(c * half, half)
    pl.semaphore_wait(barrier, 4 + len(along))
    d_n = put(rin.at[0, mine, span(z)], rin.at[1, mine, span(z)], Z)
    load_o.wait()
    weigh(c * half, half, 1, stage(2))
    d_o = put(stg.at[2, :, span(z)], og.at[1, mine, span(z)], Z)
    x_n = put(rin.at[0, mine, :], rin.at[2, mine, :], X)
    y_n = put(rin.at[0, mine, :], rin.at[3, mine, :], Y)
    weigh(c * half, half, 2, stage(0))
    x_o = put(stg.at[0], og.at[2, mine, :], X)
    weigh(c * half, half, 3, stage(1))
    y_o = put(stg.at[1], og.at[3, mine, :], Y)

    def spread(buf):
        block = buf.at[1, mine, span(z)]
        return line_put(block) + [put(block, block, across)]

    def collect(buf, copies, i):
        copies[i].wait_recv()
        block = buf.at[1, mine, span(downs[i])]
        return put(block, block, across)

    def forward(buf, slot):
        block = buf.at[slot, mine, :]
        return put(block, block, across)

    d_n.wait_recv()
    n_spread = spread(rin)
    normalize((1 - c) * half, half)
    weigh(0, count, 0, own_write)
    d_o.wait_recv()
    o_spread = spread(og)

    heads_here = decay_ref.shape[0]
    head_width = query.shape[1] // heads_here
    later = lax.broadcasted_iota(jnp.int32, (count, count), 0)
    lower = (later >= lax.broadcasted_iota(jnp.int32, (count, count), 1)).astype(jnp.float32)
    running = lax.dot_general(lower, decay_ref[...], (((1,), (1,)), ((), ())), **exact)
    load_query.wait()
    for h in range(heads_here):
        cols = slice(h * head_width, (h + 1) * head_width)
        fq_all[0, :, cols] = (
            jnp.exp(running[:, h : h + 1]) * query[:, cols].astype(jnp.float32)
        ).astype(jnp.bfloat16)
    ends_all[0] = jnp.zeros((8, 128), jnp.float32)
    ends_all[0, :, :heads_here] = jnp.broadcast_to(running[count - 1 :, :], (8, heads_here))
    load_outs.wait()
    extras = []
    for slot, target in ((1, Z), (2, X), (3, Y)):
        for buf in (ends_all, fq_all):
            extras.append(put(buf.at[0], buf.at[slot], target))

    for copy in load_w:
        copy.wait()

    def gates(slots, rows):
        lhs = rin[slots].reshape(rows, width)
        pre[slots, :, :feats] = jnp.dot(
            lhs, wg[...], preferred_element_type=jnp.float32
        ).reshape(-1, count, feats)
        pre[slots, :, feats:] = jnp.dot(
            lhs, wu[...], preferred_element_type=jnp.float32
        ).reshape(-1, count, feats)

    def hidden_grads(slots, rows):
        lhs = og[slots].reshape(rows, width)
        hgrad[slots] = contract_cols(lhs, wd[...]).reshape(-1, count, feats)

    def activations(s):
        hidden, pullback = jax.vjp(activate, pre[s, :, :feats], pre[s, :, feats:])
        gate_back, up_back = pullback(hgrad[s])
        both = gate_back * pre[s, :, :feats] + up_back * pre[s, :, feats:]
        mrow[0, s] = lax.dot_general(
            jnp.ones((8, feats), jnp.float32), both, (((1,), (1,)), ((), ())), **exact
        )
        hid[s] = hidden.astype(jnp.bfloat16)
        back[s, :, :feats] = gate_back.astype(jnp.bfloat16)
        back[s, :, feats:] = up_back.astype(jnp.bfloat16)

    def part_step(slots, rows, cols):
        lhs = back[slots].reshape(rows, 2 * feats)
        piece = contract_cols(lhs[:, :feats], wg[cols, :]) + contract_cols(
            lhs[:, feats:], wu[cols, :]
        )
        part[slots, :, cols] = piece.astype(jnp.bfloat16).reshape(-1, count, quarter)

    def pair_step(s, cols):
        def step(i, carry):
            r = pl.ds(pl.multiple_of(c * half + i * ROWS, ROWS), ROWS)
            q = pl.ds(pl.multiple_of(i * ROWS, ROWS), ROWS)
            total = part[s, r, cols].astype(jnp.float32) + pin[s, q, cols].astype(jnp.float32)
            part[s, r, cols] = total.astype(jnp.bfloat16)
            return carry

        lax.fori_loop(0, half // ROWS, step, 0)

    gates(slice(0, 1), count)
    hidden_grads(slice(0, 1), count)
    activations(0)

    def own_step(n, carry):
        part_step(slice(0, 1), count, span(n))
        return carry

    lax.fori_loop(0, depth, own_step, 0)
    swap_own = put(part.at[0, theirs, :], pin.at[0], across)

    rest = (segs - 1) * count
    x_n.wait_recv()
    f = [forward(rin, 2)]
    y_n.wait_recv()
    f.append(forward(rin, 3))
    for i in range(depth - 1):
        f.append(collect(rin, n_spread, i))
    n_spread[-1].wait_recv()
    for copy in f:
        copy.wait_recv()
    gates(slice(1, segs), rest)
    f = []
    for i in range(depth - 1):
        f.append(collect(og, o_spread, i))
    x_o.wait_recv()
    f.append(forward(og, 2))
    y_o.wait_recv()
    f.append(forward(og, 3))
    o_spread[-1].wait_recv()
    for copy in f:
        copy.wait_recv()

    def pair(s, swap, extra=()):
        swap.wait_recv()

        def step(i, carry):
            r = pl.ds(pl.multiple_of(c * half + i * ROWS, ROWS), ROWS)
            q = pl.ds(pl.multiple_of(i * ROWS, ROWS), ROWS)
            total = part[s, r, :].astype(jnp.float32) + pin[s, q, :].astype(jnp.float32)
            for ref in extra:
                total = total + ref[q, :].astype(jnp.float32)
            part[s, r, :] = total.astype(jnp.bfloat16)
            return carry

        lax.fori_loop(0, half // ROWS, step, 0)

    line_rows = rz1.shape[1]
    on_line = pl.ds(pl.multiple_of(c * half, ROWS), line_rows)
    direct = pl.ds(pl.multiple_of(c * half + line_rows, ROWS), half - line_rows)
    order = [span(q) for q in ups] + [span(z)]
    swaps, x_p, y_p, dd_p, d_z = [], [], [], [], []

    def advance(n):
        cols = order[n]
        for copy in swaps[n]:
            copy.wait_recv()
        pair_step(2, cols)
        x_p.append(put(part.at[2, mine, cols], rx.at[:, cols], X))
        pair_step(3, cols)
        y_p.append(put(part.at[3, mine, cols], ry.at[:, cols], Y))
        pair_step(1, cols)
        dd_p.append(put(part.at[1, direct, cols], rdd.at[:, cols], Z))
        if n < depth - 1:
            d_z.append(put(part.at[1, on_line, cols], rz1.at[n], along[n]))

    hidden_grads(slice(1, segs), rest)
    for slot in range(1, segs):
        activations(slot)
    m_pair = put(mrow.at[0], mrow.at[1], across)
    for n, cols in enumerate(order):
        part_step(slice(1, segs), rest, cols)
        swaps.append(
            [
                put(part.at[slot, theirs, cols], pin.at[slot, :, cols], across)
                for slot in (2, 3, 1)
            ]
        )
        if n == 1:
            m_pair.wait_recv()
            mrow[2] = mrow[0] + mrow[1]
            m_side = [
                put(mrow.at[2, slot], mland.at[slot - 1], target)
                for slot, target in ((1, Z), (2, X), (3, Y))
            ]
        if n >= 2:
            advance(n - 2)
    for n in range(depth - 2, depth):
        advance(n)

    def weight_step(n, carry):
        cols = pl.ds(pl.multiple_of(n * 512, 128), 512)
        block = contract_rows(rin[:, :, cols].reshape(segs * count, 512), back[...].reshape(segs * count, 2 * feats))
        gout[cols, :] = block[:, :feats].astype(jnp.bfloat16)
        uout[cols, :] = block[:, feats:].astype(jnp.bfloat16)
        return carry

    lax.fori_loop(0, width // 512, weight_step, 0)
    store(gout, gate_out)
    store(uout, up_out)

    def line_step(i, carry):
        q = pl.ds(pl.multiple_of(i * ROWS, ROWS), ROWS)
        r = pl.ds(pl.multiple_of(c * half + i * ROWS, ROWS), ROWS)
        total = part[1, r, span(z)].astype(jnp.float32)
        for k in range(depth - 1):
            total = total + rz1[k, q, :].astype(jnp.float32)
        sd[q, :] = total.astype(jnp.bfloat16)
        return carry

    swap_own.wait_recv()
    own_z = []
    for n, cols in enumerate(order):
        if n == depth - 1:
            for copy in d_z:
                copy.wait_recv()
            lax.fori_loop(0, line_rows // ROWS, line_step, 0)
            d_p = put(sd, rd, Z)
            for slot, target in ((1, Z), (2, X), (3, Y)):
                extras.append(put(outs_all.at[0], outs_all.at[slot], target))
        for copies in (x_p, y_p, dd_p):
            copies[n].wait_recv()

        def step(i, carry):
            r = pl.ds(pl.multiple_of(c * half + i * ROWS, ROWS), ROWS)
            q = pl.ds(pl.multiple_of(i * ROWS, ROWS), ROWS)
            total = part[0, r, cols].astype(jnp.float32)
            for ref in (pin.at[0], rx, ry):
                total = total + ref[q, cols].astype(jnp.float32)
            part[0, r, cols] = total.astype(jnp.bfloat16)
            return carry

        def direct_step(i, carry):
            r = pl.ds(pl.multiple_of(c * half + i * ROWS, ROWS), ROWS)
            q = pl.ds(pl.multiple_of(i * ROWS, ROWS), ROWS)
            u = pl.ds(pl.multiple_of(i * ROWS - line_rows, ROWS), ROWS)
            total = part[0, r, cols].astype(jnp.float32)
            for ref in (pin.at[0], rx, ry):
                total = total + ref[q, cols].astype(jnp.float32)
            total = total + rdd[u, cols].astype(jnp.float32)
            part[0, r, cols] = total.astype(jnp.bfloat16)
            return carry

        lax.fori_loop(0, line_rows // ROWS, step, 0)
        lax.fori_loop(line_rows // ROWS, half // ROWS, direct_step, 0)
        if n == 0:
            total = mrow[2, 0]
            for k, copy in enumerate(m_side):
                copy.wait_recv()
                total = total + mland[k]
            msend[...] = total
            m_z = [put(msend, mz.at[i], along[i]) for i in range(depth - 1)]
        if n < depth - 1:
            own_z.append(put(part.at[0, mine, cols], rz2.at[n], along[n]))

    def down_step(n, carry):
        cols = pl.ds(pl.multiple_of(n * 512, 128), 512)
        block = contract_rows(
            hid[...].reshape(segs * count, feats), og[:, :, cols].reshape(segs * count, 512)
        )
        dout[:, cols] = block.astype(jnp.bfloat16)
        return carry

    lax.fori_loop(0, width // 512, down_step, 0)
    store(dout, down_out)

    d_p.wait_recv()

    total = msend[...]
    for k, copy in enumerate(m_z):
        copy.wait_recv()
        total = total + mz[k]
    first = lax.broadcasted_iota(jnp.int32, (8, 128), 0) == 0
    means[...] = lax.dot_general(
        total / width, first.astype(jnp.float32), (((0,), (0,)), ((), ())), **exact
    )
    for copy in own_z:
        copy.wait_recv()

    def resid_step(i, u):
        q = pl.ds(pl.multiple_of(i * ROWS, ROWS), ROWS)
        r = pl.ds(pl.multiple_of(c * half + i * ROWS, ROWS), ROWS)
        total = part[0, r, span(z)].astype(jnp.float32)
        for k in range(depth - 1):
            total = total + rz2[k, q, :].astype(jnp.float32)
        if u is not None:
            total = total + rd[q, :].astype(jnp.float32)
        weighted = gain_ref[:, span(z)] * total
        inverse = inv[r, 0:1]
        scaled = raw_r[r, span(z)].astype(jnp.float32) * inverse
        grad = raw_o[r, span(z)].astype(jnp.float32) + inverse * (weighted - scaled * means[r, 0:1])
        rg[r, span(z)] = grad.astype(jnp.bfloat16)

    def resid_line(i, carry):
        resid_step(i, True)
        return carry

    def resid_direct(i, carry):
        resid_step(i, None)
        return carry

    lax.fori_loop(0, line_rows // ROWS, resid_line, 0)
    lax.fori_loop(line_rows // ROWS, half // ROWS, resid_direct, 0)
    block = rg.at[mine, span(z)]
    g_z = line_put(block)
    g_f = [put(block, block, across)]
    col_copies = [
        (t, slot, remote(rg.at[mine, span(t)], col.at[slot, mine, :], target))
        for t, slot, target in ((gd, 1, Z), (gx, 2, X), (gy, 3, Y))
    ]

    def send_columns(q):
        for t, _, copy in col_copies:

            @pl.when(q == t)
            def _():
                copy.start()

    send_columns(z)
    for i in range(depth - 1):
        g_z[i].wait_recv()
        block = rg.at[mine, span(downs[i])]
        g_f.append(put(block, block, across))
        send_columns(downs[i])
    for copy in g_f:
        copy.wait_recv()
    load_op.wait()
    hga[0] = contract_cols(rg[...], op[...]).astype(jnp.bfloat16)
    heads = [put(hga.at[0], hga.at[slot], t) for slot, t in ((1, Z), (2, X), (3, Y))]
    col[0] = rg[:, span(g)]
    col_f = []
    for _, slot, copy in col_copies:
        copy.wait_recv()
        col_f.append(forward(col, slot))
    for copy in extras:
        copy.wait_recv()
    store(outs_all, outs_out)
    store(fq_all, fq_out)
    store(ends_all, ends_out)
    for copy in col_f:
        copy.wait_recv()
    store(col, col_out)
    for copy in heads:
        copy.wait_recv()
    store(hga, hg_out)
    for copy in sends:
        copy.wait_send()
    for copy in stores:
        copy.wait()


def square_call(segs, raw_r, raw_o, ids, scale, decay, gain, wg, wu, wd, op, outs, query):
    count, width = raw_r.shape
    feats, heads = wg.shape[1], outs.shape[1]
    half, quarter = count // CORES, width // segs
    line = half * 3 // 5 // ROWS * ROWS
    bf16, f32 = jnp.bfloat16, jnp.float32
    any_spec = pl.BlockSpec(memory_space=pl.ANY)
    vmem_spec = pl.BlockSpec(memory_space=pltpu.VMEM)
    shape = jax.ShapeDtypeStruct
    flops = 2 * segs * count * width * feats * 8
    return pl.pallas_call(
        square_kernel,
        out_shape=(
            shape((width, feats), bf16),
            shape((width, feats), bf16),
            shape((feats, width), bf16),
            shape((segs, count, quarter), bf16),
            shape((segs, count, heads), bf16),
            shape((segs, count, heads), bf16),
            shape((segs, count, heads), bf16),
            shape((segs, 8, 128), f32),
        ),
        in_specs=[any_spec] * 2 + [vmem_spec] * 4 + [any_spec] * 6,
        out_specs=(any_spec,) * 8,
        scratch_shapes=[
            pltpu.VMEM((count, width), bf16),
            pltpu.VMEM((count, width), bf16),
            pltpu.VMEM((segs, count, width), bf16),
            pltpu.VMEM((segs, count, width), bf16),
            pltpu.VMEM((3, half, width), bf16),
            pltpu.VMEM((width, feats), bf16),
            pltpu.VMEM((width, feats), bf16),
            pltpu.VMEM((feats, width), bf16),
            pltpu.VMEM((heads, width), bf16),
            pltpu.VMEM((segs, count, width), bf16),
            pltpu.VMEM((segs, half, width), bf16),
            pltpu.VMEM((segs, count, feats), bf16),
            pltpu.VMEM((segs, count, 2 * feats), bf16),
            pltpu.VMEM((segs, count, 2 * feats), f32),
            pltpu.VMEM((segs, count, feats), f32),
            pltpu.VMEM((count, heads), bf16),
            pltpu.VMEM((half, width), bf16),
            pltpu.VMEM((half, width), bf16),
            pltpu.VMEM((half - line, width), bf16),
            pltpu.VMEM((segs - 1, line, quarter), bf16),
            pltpu.VMEM((line, quarter), bf16),
            pltpu.VMEM((line, quarter), bf16),
            pltpu.VMEM((segs - 1, half, quarter), bf16),
            pltpu.VMEM((count, 128), f32),
            pltpu.VMEM((count, 128), f32),
            pltpu.VMEM((count, 128), f32),
            pltpu.VMEM((3, segs, 8, count), f32),
            pltpu.VMEM((segs - 1, 8, count), f32),
            pltpu.VMEM((8, count), f32),
            pltpu.VMEM((segs - 1, 8, count), f32),
            pltpu.VMEM((count, width), bf16),
            pltpu.VMEM((segs, count, quarter), bf16),
            pltpu.VMEM((segs, count, heads), bf16),
            pltpu.VMEM((segs, count, heads), bf16),
            pltpu.VMEM((segs, count, heads), bf16),
            pltpu.VMEM((segs, 8, 128), f32),
            pltpu.VMEM((width, feats), bf16),
            pltpu.VMEM((width, feats), bf16),
            pltpu.VMEM((feats, width), bf16),
            pltpu.SemaphoreType.DMA((96,)),
            pltpu.SemaphoreType.DMA((96,)),
            pltpu.SemaphoreType.DMA((8,)),
            pltpu.SemaphoreType.DMA((8,)),
        ],
        compiler_params=pltpu.CompilerParams(
            collective_id=0, has_side_effects=True, vmem_limit_bytes=VMEM_LIMIT
        ),
        cost_estimate=pl.CostEstimate(flops=flops, bytes_accessed=40000000, transcendentals=0),
    )(raw_r, raw_o, ids, scale, decay, gain, wg, wu, wd, op, outs, query)


def tail_kernel(
    gate_in,
    up_in,
    down_in,
    col_hbm,
    hg_hbm,
    outs_hbm,
    fq_hbm,
    ends_hbm,
    query_hbm,
    key_hbm,
    value_hbm,
    entry_hbm,
    decay_ref,
    gate_out,
    up_out,
    down_out,
    proj_out,
    query_out,
    key_out,
    value_out,
    gate,
    up,
    down,
    col,
    hga,
    outs,
    fqa,
    ends,
    query,
    key,
    value,
    entry,
    proj,
    query_grad,
    key_grad,
    value_grad,
    load_sems,
    store_sems,
):
    segs, count, quarter = col.shape
    heads_here = decay_ref.shape[0]
    head_width = query.shape[1] // heads_here
    channels = query.shape[1]
    loads = []

    def load(src, dst):
        copy = pltpu.make_async_copy(src, dst, load_sems.at[len(loads)])
        copy.start()
        loads.append(copy)
        return copy

    stores = []

    def store(src, dst):
        copy = pltpu.make_async_copy(src, dst, store_sems.at[len(stores)])
        copy.start()
        stores.append(copy)

    early = [
        load(*pair)
        for pair in (
            (query_hbm, query),
            (key_hbm, key),
            (value_hbm, value),
            (hg_hbm, hga),
            (fq_hbm, fqa),
            (ends_hbm, ends),
            (entry_hbm, entry),
        )
    ]
    load_col = [load(col_hbm, col), load(outs_hbm, outs)]
    through = [
        (load(gate_in, gate), gate, gate_out),
        (load(up_in, up), up, up_out),
        (load(down_in, down), down, down_out),
    ]
    g = lax.axis_index("sp")
    gy_, gx_ = g // 2, g % 2
    seg_of = [
        g,
        (1 - gy_) * 2 + (1 - gx_),
        gy_ * 2 + (1 - gx_),
        (1 - gy_) * 2 + gx_,
    ]
    row = lax.broadcasted_iota(jnp.int32, (count, count), 0)
    column = lax.broadcasted_iota(jnp.int32, (count, count), 1)
    causal = row >= column
    decay = decay_ref[...]
    exact = dict(preferred_element_type=jnp.float32, precision=lax.Precision.HIGHEST)
    lower = causal.astype(jnp.float32)
    running = lax.dot_general(lower, decay, (((1,), (1,)), ((), ())), **exact)
    across = lax.dot_general(decay, lower, (((1,), (1,)), ((), ())), **exact)
    key_scale = head_width ** (-0.5)
    bf16 = jnp.bfloat16
    for copy in early:
        copy.wait()

    def mul(left, right):
        return jnp.dot(left, right, preferred_element_type=jnp.float32)

    for h in range(heads_here):
        cols = slice(h * head_width, (h + 1) * head_width)
        run = running[:, h : h + 1]
        from_start = jnp.exp(run)
        to_end = jnp.exp(running[count - 1 :, h : h + 1] - run)
        spread = jnp.where(causal, run - across[h : h + 1, :], 0.0)
        weights = jnp.where(causal, jnp.exp(spread), 0.0)
        state = jnp.zeros((head_width, head_width), jnp.float32)
        for j in range(1, segs):
            between = jnp.zeros((1, 1), jnp.float32)
            for i in range(1, segs):
                if i != j:
                    inside = (seg_of[i] > g) & (seg_of[i] < seg_of[j])
                    between = between + jnp.where(inside, ends[i, 0:1, h : h + 1], 0.0)
            passed = jnp.where(seg_of[j] > g, jnp.exp(between), 0.0)
            state = state + passed * contract_rows(fqa[j, :, cols], hga[j, :, cols])
        state = state.astype(bf16)
        grad = hga[0, :, cols]
        q, k, v = query[:, cols], key[:, cols], value[:, cols]
        grad_scores = (contract_cols(grad, v) * weights).astype(bf16)
        key_scores = (contract_cols(q, k) * weights).astype(bf16)
        query_grad[:, cols] = (
            key_scale
            * (mul(grad_scores, k) + from_start * contract_cols(grad, entry[h].astype(bf16)))
        ).astype(bf16)
        key_grad[:, cols] = (
            key_scale * (contract_rows(grad_scores, q) + to_end * contract_cols(v, state))
        ).astype(bf16)
        value_grad[:, cols] = (
            key_scale * (contract_rows(key_scores, grad) + to_end * mul(k, state))
        ).astype(bf16)
    store(query_grad, query_out)
    store(key_grad, key_out)
    store(value_grad, value_out)
    for copy, src, dst in through:
        copy.wait()
        store(src, dst)
    for copy in load_col:
        copy.wait()
    right = outs[...].reshape(segs * count, channels)
    for n in range(quarter // 256):
        cols = slice(n * 256, (n + 1) * 256)
        proj[cols, :] = contract_rows(col[:, :, cols].reshape(segs * count, 256), right)
        store(proj.at[cols, :], proj_out.at[cols, :])
    for copy in stores:
        copy.wait()


def tail_call(gate, up, down, col, hga, outs, fqa, ends, query, key, value, entry, decay):
    segs, count, quarter = col.shape
    channels = query.shape[1]
    any_spec = pl.BlockSpec(memory_space=pl.ANY)
    shape = jax.ShapeDtypeStruct
    rows = shape((count, channels), jnp.bfloat16)
    proj = shape((quarter, channels), jnp.float32)
    kept = [gate, up, down, col, hga, outs, fqa, ends, query, key, value, entry]
    results = [proj, rows, rows, rows]
    return pl.pallas_call(
        tail_kernel,
        out_shape=tuple(shape(a.shape, a.dtype) for a in (gate, up, down)) + tuple(results),
        in_specs=[any_spec] * len(kept) + [pl.BlockSpec(memory_space=pltpu.VMEM)],
        out_specs=(any_spec,) * 7,
        scratch_shapes=[pltpu.VMEM(a.shape, a.dtype) for a in kept + results]
        + [pltpu.SemaphoreType.DMA((12,)), pltpu.SemaphoreType.DMA((16,))],
        compiler_params=pltpu.CompilerParams(vmem_limit_bytes=VMEM_LIMIT),
        cost_estimate=pl.CostEstimate(
            flops=2 * segs * count * quarter * channels,
            bytes_accessed=30000000,
            transcendentals=0,
        ),
    )(*kept, decay)


def local_square(
    residual_mid,
    out_grad,
    norm_gain,
    expert_ids,
    expert_weights,
    gate_proj,
    up_proj,
    down_proj,
    out_proj,
    query_rows,
    key_rows,
    value_rows,
    retention_out,
    log_decay,
    entry_state,
):
    width = residual_mid.shape[1]
    segs = lax.axis_size("sp")
    gate_grad, up_grad, down_grad, columns, grads, outs, fqs, ends = square_call(
        segs,
        residual_mid,
        out_grad,
        expert_ids.T,
        expert_weights.T,
        log_decay.T,
        norm_gain.reshape(1, width),
        gate_proj[0],
        up_proj[0],
        down_proj[0],
        out_proj,
        retention_out,
        query_rows,
    )
    gate_grad, up_grad, down_grad, proj_grad, query_grad, key_grad, value_grad = tail_call(
        gate_grad,
        up_grad,
        down_grad,
        columns,
        grads,
        outs,
        fqs,
        ends,
        query_rows,
        key_rows,
        value_rows,
        entry_state[0],
        log_decay.T,
    )
    return (
        gate_grad[None],
        up_grad[None],
        down_grad[None],
        proj_grad,
        query_grad,
        key_grad,
        value_grad,
    )


def solution(mesh):
    segs, split = mesh.shape["sp"], mesh.shape["tp"]
    fine = Mesh(mesh.devices.reshape(segs, split // CORES, CORES), ("sp", "z", "core"))
    tp = ("z", "core")
    placed = (
        P("sp", None),
        P("sp", None),
        P(),
        P("sp", None),
        P("sp", None),
        P("sp", None, tp),
        P("sp", None, tp),
        P("sp", tp, None),
        P(tp, None),
        P("sp", tp),
        P("sp", tp),
        P("sp", tp),
        P("sp", tp),
        P("sp", tp),
        P("sp", tp, None, None),
    )
    fast = segs == 4 and split == segs * CORES
    return jax.shard_map(
        local_square if fast else local_general,
        mesh=fine,
        in_specs=placed,
        out_specs=(
            P("sp", None, tp),
            P("sp", None, tp),
            P("sp", tp, None),
            P("sp", tp),
            P("sp", tp),
            P("sp", tp),
            P("sp", tp),
        ),
        check_vma=False,
    )
```

```python
import jax
import jax.numpy as jnp
from jax import lax
from jax.experimental import pallas as pl
from jax.experimental.pallas import tpu as pltpu
from jax.sharding import Mesh, PartitionSpec as P

CLAMP_LIMIT = 7.0
GATE_ALPHA = 1.702
NORM_EPSILON = 1e-05
CORES = 2
SWAP = [(0, 1), (1, 0)]


def activate(gate_pre, up_pre):
    gate_clamped = jnp.minimum(gate_pre, CLAMP_LIMIT)
    up_clamped = jnp.clip(up_pre, -CLAMP_LIMIT, CLAMP_LIMIT)
    return (up_clamped + 1.0) * gate_clamped * jax.nn.sigmoid(GATE_ALPHA * gate_clamped)


def contract_rows(left, right):
    return lax.dot_general(
        left, right, (((0,), (0,)), ((), ())), preferred_element_type=jnp.float32
    )


def contract_cols(left, right):
    return lax.dot_general(
        left, right, (((1,), (1,)), ((), ())), preferred_element_type=jnp.float32
    )


def dots(spec, left, right):
    return jnp.einsum(
        spec,
        left.astype(jnp.bfloat16),
        right.astype(jnp.bfloat16),
        preferred_element_type=jnp.float32,
    )


def local_general(
    residual_mid,
    out_grad,
    norm_gain,
    expert_ids,
    expert_weights,
    gate_proj,
    up_proj,
    down_proj,
    out_proj,
    query_rows,
    key_rows,
    value_rows,
    retention_out,
    log_decay,
    entry_state,
):
    token_count, width = residual_mid.shape
    segs = lax.axis_size("sp")
    depth = lax.axis_size("z")
    seg = lax.axis_index("sp")
    core = lax.axis_index("core")
    half = token_count // CORES
    share = half // depth

    def rows_of(array, start, count):
        return lax.dynamic_slice_in_dim(array, start, count, axis=0)

    def normalize(rows):
        wide = rows.astype(jnp.float32)
        inverse = lax.rsqrt(jnp.mean(wide * wide, axis=1, keepdims=True) + NORM_EPSILON)
        return wide * inverse, inverse

    grad_own = lax.all_gather(rows_of(out_grad, core * half, half), "sp").reshape(-1, width)
    normed_half = (normalize(rows_of(residual_mid, core * half, half))[0] * norm_gain).astype(
        jnp.bfloat16
    )
    normed_own = lax.all_gather(normed_half, "sp").reshape(-1, width)
    grad_other = lax.ppermute(grad_own, "core", SWAP)
    normed_other = lax.ppermute(normed_own, "core", SWAP)

    experts = jnp.arange(segs, dtype=jnp.int32)
    route = jnp.sum(
        jnp.where(expert_ids.T[None] == experts[:, None, None], expert_weights.T[None], 0.0), axis=1
    )
    heads_here = log_decay.shape[1]
    small = jnp.concatenate([route.reshape(-1), jnp.sum(log_decay, axis=0)])
    smalls = lax.all_gather(small, "sp")
    routes = smalls[:, : segs * token_count].reshape(segs, segs, token_count)
    seg_decay = smalls[:, segs * token_count :]
    here = lax.dynamic_index_in_dim(routes, seg, axis=1, keepdims=False)
    here = here.reshape(segs, CORES, half)
    weight_own = lax.dynamic_index_in_dim(here, core, axis=1, keepdims=False).reshape(-1, 1)
    weight_other = lax.dynamic_index_in_dim(here, 1 - core, axis=1, keepdims=False).reshape(-1, 1)

    gate_weight = gate_proj[0]
    up_weight = up_proj[0]
    down_weight = down_proj[0]

    def expert(rows_in, rows_out, weight):
        rows_grad = (weight * rows_out.astype(jnp.float32)).astype(jnp.bfloat16)
        gate_pre = jnp.dot(rows_in, gate_weight, preferred_element_type=jnp.float32)
        up_pre = jnp.dot(rows_in, up_weight, preferred_element_type=jnp.float32)
        hidden, pullback = jax.vjp(activate, gate_pre, up_pre)
        gate_back, up_back = pullback(contract_cols(rows_grad, down_weight))
        gate_back = gate_back.astype(jnp.bfloat16)
        up_back = up_back.astype(jnp.bfloat16)
        part = contract_cols(gate_back, gate_weight) + contract_cols(up_back, up_weight)
        return part, rows_grad, hidden.astype(jnp.bfloat16), gate_back, up_back

    part_own, cot_own, hidden_own, gate_back_own, up_back_own = expert(
        normed_own, grad_own, weight_own
    )
    part_other, cot_other, hidden_other, gate_back_other, up_back_other = expert(
        normed_other, grad_other, weight_other
    )
    part_got = lax.ppermute(part_other.astype(jnp.bfloat16), "core", SWAP)
    part_pair = (part_own + part_got.astype(jnp.float32)).astype(jnp.bfloat16)
    part_seg = lax.psum_scatter(
        part_pair.reshape(segs, half, width), "sp", scatter_dimension=0, tiled=False
    )
    mixed_grad = lax.psum_scatter(
        part_seg.reshape(depth, share, width), "z", scatter_dimension=0, tiled=False
    ).astype(jnp.float32)

    down_grad = (contract_rows(hidden_own, cot_own) + contract_rows(hidden_other, cot_other)).astype(
        jnp.bfloat16
    )[None]
    gate_grad = (
        contract_rows(normed_own, gate_back_own) + contract_rows(normed_other, gate_back_other)
    ).astype(jnp.bfloat16)[None]
    up_grad = (
        contract_rows(normed_own, up_back_own) + contract_rows(normed_other, up_back_other)
    ).astype(jnp.bfloat16)[None]

    start = core * half + lax.axis_index("z") * share
    scaled, inverse = normalize(rows_of(residual_mid, start, share))
    weighted = norm_gain * mixed_grad
    inner = jnp.mean(scaled * weighted, axis=1, keepdims=True)
    resid_part = (
        rows_of(out_grad, start, share).astype(jnp.float32)
        + inverse * (weighted - scaled * inner)
    ).astype(jnp.bfloat16)
    resid_grad = lax.all_gather(resid_part, ("core", "z"), axis=0, tiled=False).reshape(
        token_count, width
    )
    columns = lax.all_to_all(
        resid_part.reshape(share, segs, width // segs).transpose(1, 0, 2),
        "sp",
        split_axis=0,
        concat_axis=0,
        tiled=True,
    )
    columns = lax.all_gather(columns, ("core", "z"), axis=0, tiled=False).reshape(
        segs * token_count, -1
    )
    outs = lax.all_gather(retention_out, "sp")
    outs = outs.reshape(segs, CORES * depth, share, -1).transpose(1, 0, 2, 3)
    outs = outs.reshape(segs * token_count, -1)
    proj_grad = contract_rows(columns, outs)

    head_grad = contract_cols(resid_grad, out_proj).astype(jnp.bfloat16)

    def split_heads(rows):
        return rows.reshape(token_count, heads_here, -1).transpose(1, 0, 2)

    queries = split_heads(query_rows)
    key_heads = split_heads(key_rows)
    value_heads = split_heads(value_rows)
    grad_heads = split_heads(head_grad)
    key_scale = queries.shape[2] ** (-0.5)
    running = jnp.cumsum(log_decay, axis=0).T
    from_start = jnp.exp(running)
    to_end = jnp.exp(running[:, -1:] - running)
    position = jnp.arange(token_count, dtype=jnp.int32)
    causal = (position[:, None] >= position[None, :])[None]
    spread = jnp.where(causal, running[:, :, None] - running[:, None, :], 0.0)
    weights = jnp.where(causal, jnp.exp(spread), 0.0)
    local_state = dots("htk,hte->hke", from_start[:, :, None] * queries, grad_heads)
    states = lax.all_gather(local_state.astype(jnp.bfloat16), "sp")
    order = jnp.arange(segs, dtype=jnp.int32)
    between = (order[None, :] > seg) & (order[None, :] < order[:, None])
    passed = jnp.exp(jnp.sum(jnp.where(between[:, :, None], seg_decay[None], 0.0), axis=1))
    passed = jnp.where(order[:, None] > seg, passed, 0.0)
    later_state = jnp.sum(passed[:, :, None, None] * states.astype(jnp.float32), axis=0)
    entry = entry_state[0]
    grad_scores = dots("hte,hse->hts", grad_heads, value_heads) * weights
    key_scores = dots("htk,hsk->hts", queries, key_heads) * weights
    query_grad = key_scale * (
        dots("hts,hsk->htk", grad_scores, key_heads)
        + from_start[:, :, None] * dots("hte,hke->htk", grad_heads, entry)
    )
    key_grad = key_scale * (
        dots("hts,htk->hsk", grad_scores, queries)
        + to_end[:, :, None] * dots("hse,hke->hsk", value_heads, later_state)
    )
    value_grad = key_scale * (
        dots("hts,hte->hse", key_scores, grad_heads)
        + to_end[:, :, None] * dots("hsk,hke->hse", key_heads, later_state)
    )

    def merge_heads(heads_rows):
        return heads_rows.transpose(1, 0, 2).reshape(token_count, -1).astype(jnp.bfloat16)

    return (
        gate_grad,
        up_grad,
        down_grad,
        proj_grad,
        merge_heads(query_grad),
        merge_heads(key_grad),
        merge_heads(value_grad),
    )


ROWS = 16
VMEM_LIMIT = 66 * 1000 * 1000
MESH_ID = pl.DeviceIdType.MESH


def square_kernel(
    raw_r_hbm,
    raw_o_hbm,
    ids_hbm,
    scale_hbm,
    decay_hbm,
    gain_hbm,
    wg_hbm,
    wu_hbm,
    wd_hbm,
    op_hbm,
    outs_hbm,
    query_hbm,
    gate_out,
    up_out,
    down_out,
    col_out,
    hg_out,
    outs_out,
    fq_out,
    ends_out,
    ids_ref,
    scale_ref,
    decay_ref,
    gain_ref,
    raw_r,
    raw_o,
    rin,
    og,
    stg,
    wg,
    wu,
    wd,
    wdt,
    wgut,
    op,
    part,
    pin,
    hid,
    back,
    pre,
    hgrad,
    slope_m,
    query,
    rx,
    ry,
    rdd,
    rz1,
    sd,
    rd,
    rz2,
    inv,
    route,
    means,
    mrow,
    mland,
    msend,
    mz,
    rg,
    col,
    hga,
    outs_all,
    fq_all,
    ends_all,
    gout,
    uout,
    dout,
    send_sems,
    recv_sems,
    load_sems,
    store_sems,
):
    segs, count, width = rin.shape
    half = count // CORES
    depth = segs
    quarter = width // depth
    feats = wg.shape[1]
    g = lax.axis_index("sp")
    z = lax.axis_index("z")
    c = lax.axis_index("core")
    gy_, gx_ = g // 2, g % 2
    gx = gy_ * 2 + (1 - gx_)
    gy = (1 - gy_) * 2 + gx_
    gd = (1 - gy_) * 2 + (1 - gx_)
    ups = [(z + i) % depth for i in range(1, depth)]
    downs = [(z + depth - i) % depth for i in range(1, depth)]
    mine = pl.ds(pl.multiple_of(c * half, ROWS), half)
    theirs = pl.ds(pl.multiple_of((1 - c) * half, ROWS), half)

    def span(index):
        return pl.ds(pl.multiple_of(index * quarter, 128), quarter)

    def dev(sp, zz, cc):
        return {"sp": sp, "z": zz, "core": cc}

    sends = []
    used = [0]

    def remote(src, dst, target):
        k = used[0]
        used[0] += 1
        copy = pltpu.make_async_remote_copy(
            src_ref=src,
            dst_ref=dst,
            send_sem=send_sems.at[k],
            recv_sem=recv_sems.at[k],
            device_id=target,
            device_id_type=MESH_ID,
        )
        sends.append(copy)
        return copy

    def put(src, dst, target):
        copy = remote(src, dst, target)
        copy.start()
        return copy

    def line_put(block):
        return [put(block, block, target) for target in along]

    loads = []

    def load(src, dst):
        copy = pltpu.make_async_copy(src, dst, load_sems.at[len(loads)])
        copy.start()
        loads.append(copy)
        return copy

    stores = []

    def store(src, dst):
        copy = pltpu.make_async_copy(src, dst, store_sems.at[len(stores)])
        copy.start()
        stores.append(copy)

    load_small = [load(ids_hbm, ids_ref), load(scale_hbm, scale_ref)]
    load_gain = load(gain_hbm, gain_ref)
    load_r = load(raw_r_hbm, raw_r)
    load_o = load(raw_o_hbm, raw_o)
    load_decay = load(decay_hbm, decay_ref)
    load_w = [load(wg_hbm, wg), load(wu_hbm, wu), load(wd_hbm, wd)]
    load_op = load(op_hbm, op)
    load_outs = load(outs_hbm, outs_all.at[0])
    load_query = load(query_hbm, query)

    X, Y, Z = dev(gx, z, c), dev(gy, z, c), dev(gd, z, c)
    across = dev(g, z, 1 - c)
    along = [dev(g, zz, c) for zz in ups]
    barrier = pltpu.get_barrier_semaphore()
    for target in [X, Y, Z, across] + along:
        pl.semaphore_signal(barrier, inc=1, device_id=target, device_id_type=MESH_ID)

    kinds = (g, gd, gx, gy)
    which = lax.broadcasted_iota(jnp.int32, (8, count), 0)
    for copy in load_small:
        copy.wait()
    table = jnp.zeros((8, count), jnp.float32)
    for k, expert in enumerate(kinds):
        chosen = jnp.where(ids_ref[...] == expert, scale_ref[...], 0.0)
        table = jnp.where(which == k, jnp.sum(chosen, axis=0, keepdims=True), table)
    unit = lax.broadcasted_iota(jnp.int32, (8, 128), 0) == lax.broadcasted_iota(
        jnp.int32, (8, 128), 1
    )
    exact = dict(preferred_element_type=jnp.float32, precision=lax.Precision.HIGHEST)
    route[...] = lax.dot_general(
        table, unit.astype(jnp.float32), (((0,), (0,)), ((), ())), **exact
    )

    def weigh(base, rows, kind, write):
        def step(i, carry):
            r = pl.ds(pl.multiple_of(base + i * ROWS, ROWS), ROWS)
            w = route[r, kind : kind + 1]
            write(i, r, (w * raw_o[r, :].astype(jnp.float32)).astype(jnp.bfloat16))
            return carry

        lax.fori_loop(0, rows // ROWS, step, 0)

    def stage(index):
        def write(i, r, value):
            stg[index, pl.ds(pl.multiple_of(i * ROWS, ROWS), ROWS), :] = value

        return write

    def own_write(i, r, value):
        og[0, r, :] = value

    def normalize(base, rows):
        def step(i, carry):
            r = pl.ds(pl.multiple_of(base + i * ROWS, ROWS), ROWS)
            wide = raw_r[r, :].astype(jnp.float32)
            inverse = lax.rsqrt(jnp.mean(wide * wide, axis=1, keepdims=True) + NORM_EPSILON)
            inv[r, :] = jnp.broadcast_to(inverse, (ROWS, 128))
            rin[0, r, :] = (wide * inverse * gain_ref[...]).astype(jnp.bfloat16)
            return carry

        lax.fori_loop(0, rows // ROWS, step, 0)

    load_gain.wait()
    load_r.wait()
    normalize(c * half, half)
    pl.semaphore_wait(barrier, 4 + len(along))
    d_n = put(rin.at[0, mine, span(z)], rin.at[1, mine, span(z)], Z)
    load_o.wait()
    weigh(c * half, half, 1, stage(2))
    d_o = put(stg.at[2, :, span(z)], og.at[1, mine, span(z)], Z)
    x_n = put(rin.at[0, mine, :], rin.at[2, mine, :], X)
    y_n = put(rin.at[0, mine, :], rin.at[3, mine, :], Y)
    weigh(c * half, half, 2, stage(0))
    line_rows = rz1.shape[1]
    cuts = [(0, line_rows), (line_rows, half - line_rows)]

    def rows_of(cut):
        return pl.ds(pl.multiple_of(c * half + cut[0], ROWS), cut[1])

    def send_cut(index, slot, target, cut):
        return put(stg.at[index, slice(cut[0], cut[0] + cut[1]), :], og.at[slot, rows_of(cut), :], target)

    x_o = [send_cut(0, 2, X, cut) for cut in cuts]
    weigh(c * half, half, 3, stage(1))
    y_o = [send_cut(1, 3, Y, cut) for cut in cuts]

    def spread(buf):
        block = buf.at[1, mine, span(z)]
        return line_put(block) + [put(block, block, across)]

    def collect(buf, copies, i):
        copies[i].wait_recv()
        block = buf.at[1, mine, span(downs[i])]
        return put(block, block, across)

    def forward(buf, slot):
        block = buf.at[slot, mine, :]
        return put(block, block, across)

    d_n.wait_recv()
    n_spread = spread(rin)
    normalize((1 - c) * half, half)
    weigh(0, count, 0, own_write)
    d_o.wait_recv()
    o_spread = spread(og)

    load_decay.wait()
    heads_here = decay_ref.shape[0]
    head_width = query.shape[1] // heads_here
    later = lax.broadcasted_iota(jnp.int32, (count, count), 0)
    lower = (later >= lax.broadcasted_iota(jnp.int32, (count, count), 1)).astype(jnp.float32)
    running = lax.dot_general(lower, decay_ref[...], (((1,), (1,)), ((), ())), **exact)
    load_query.wait()
    for h in range(heads_here):
        cols = slice(h * head_width, (h + 1) * head_width)
        fq_all[0, :, cols] = (
            jnp.exp(running[:, h : h + 1]) * query[:, cols].astype(jnp.float32)
        ).astype(jnp.bfloat16)
    ends_all[0] = jnp.zeros((8, 128), jnp.float32)
    ends_all[0, :, :heads_here] = jnp.broadcast_to(running[count - 1 :, :], (8, heads_here))
    load_outs.wait()
    extras = []
    for slot, target in ((1, Z), (2, X), (3, Y)):
        for buf in (ends_all, fq_all):
            extras.append(put(buf.at[0], buf.at[slot], target))

    for copy in load_w:
        copy.wait()

    def gates(slots, rows):
        lhs = rin[slots].reshape(rows, width)
        pre[slots, :, :feats] = jnp.dot(
            lhs, wg[...], preferred_element_type=jnp.float32
        ).reshape(-1, count, feats)
        pre[slots, :, feats:] = jnp.dot(
            lhs, wu[...], preferred_element_type=jnp.float32
        ).reshape(-1, count, feats)

    def slopes(s):
        gate_pre, up_pre = pre[s, :, :feats], pre[s, :, feats:]
        hidden, pullback = jax.vjp(activate, gate_pre, up_pre)
        gate_slope, up_slope = pullback(jnp.ones_like(hidden))
        hid[s] = hidden.astype(jnp.bfloat16)
        slope_m[s] = gate_slope * gate_pre + up_slope * up_pre
        pre[s, :, :feats] = gate_slope
        pre[s, :, feats:] = up_slope

    def backward(s):
        grad = hgrad[s]
        mrow[0, s] = lax.dot_general(
            jnp.ones((8, feats), jnp.float32),
            grad * slope_m[s],
            (((1,), (1,)), ((), ())),
            **exact,
        )
        back[s, :, :feats] = (grad * pre[s, :, :feats]).astype(jnp.bfloat16)
        back[s, :, feats:] = (grad * pre[s, :, feats:]).astype(jnp.bfloat16)

    def pair_step(s, cols):
        def step(i, carry):
            r = pl.ds(pl.multiple_of(c * half + i * ROWS, ROWS), ROWS)
            q = pl.ds(pl.multiple_of(i * ROWS, ROWS), ROWS)
            total = part[s, r, cols].astype(jnp.float32) + pin[s, q, cols].astype(jnp.float32)
            part[s, r, cols] = total.astype(jnp.bfloat16)
            return carry

        lax.fori_loop(0, half // ROWS, step, 0)

    gates(slice(0, 1), count)
    slopes(0)
    hgrad[0] = contract_cols(og[0], wd[...])
    backward(0)

    def own_step(n, carry):
        cols = span(n)
        piece = contract_cols(back[0, :, :feats], wg[cols, :]) + contract_cols(
            back[0, :, feats:], wu[cols, :]
        )
        part[0, :, cols] = piece.astype(jnp.bfloat16)
        return carry

    lax.fori_loop(0, depth, own_step, 0)
    swap_own = put(part.at[0, theirs, :], pin.at[0], across)


    def turn(n, carry):
        cols = pl.ds(pl.multiple_of(n * 512, 128), 512)
        wdt[cols, :] = wd[:, cols].T
        wgut[:feats, cols] = wg[cols, :].T
        wgut[feats:, cols] = wu[cols, :].T
        return carry

    lax.fori_loop(0, width // 512, turn, 0)
    rest = (segs - 1) * count
    x_n.wait_recv()
    f = [forward(rin, 2)]
    y_n.wait_recv()
    f.append(forward(rin, 3))
    for i in range(depth - 1):
        f.append(collect(rin, n_spread, i))
    n_spread[-1].wait_recv()
    for copy in f:
        copy.wait_recv()
    gates(slice(1, segs), rest)
    for slot in range(1, segs):
        slopes(slot)
    f = []
    for i in range(depth - 1):
        f.append(collect(og, o_spread, i))
    for k, cut in enumerate(cuts):
        for slot, copies in ((2, x_o), (3, y_o)):
            copies[k].wait_recv()
            block = og.at[slot, rows_of(cut), :]
            f.append(put(block, block, across))
    o_spread[-1].wait_recv()
    for copy in f:
        copy.wait_recv()

    def pair(s, swap, extra=()):
        swap.wait_recv()

        def step(i, carry):
            r = pl.ds(pl.multiple_of(c * half + i * ROWS, ROWS), ROWS)
            q = pl.ds(pl.multiple_of(i * ROWS, ROWS), ROWS)
            total = part[s, r, :].astype(jnp.float32) + pin[s, q, :].astype(jnp.float32)
            for ref in extra:
                total = total + ref[q, :].astype(jnp.float32)
            part[s, r, :] = total.astype(jnp.bfloat16)
            return carry

        lax.fori_loop(0, half // ROWS, step, 0)

    on_line = pl.ds(pl.multiple_of(c * half, ROWS), line_rows)
    direct = pl.ds(pl.multiple_of(c * half + line_rows, ROWS), half - line_rows)
    order = [span(q) for q in ups] + [span(z)]
    swaps, x_p, y_p, dd_p, d_z = [], [], [], [], []

    def advance(n):
        cols = order[n]
        for copy in swaps[n]:
            copy.wait_recv()
        pair_step(2, cols)
        x_p.append(put(part.at[2, mine, cols], rx.at[:, cols], X))
        pair_step(3, cols)
        y_p.append(put(part.at[3, mine, cols], ry.at[:, cols], Y))
        pair_step(1, cols)
        dd_p.append(put(part.at[1, direct, cols], rdd.at[:, cols], Z))
        if n < depth - 1:
            d_z.append(put(part.at[1, on_line, cols], rz1.at[n], along[n]))

    halves = [
        jnp.dot(
            jnp.concatenate([og[1, part_rows], og[2, part_rows], og[3, part_rows]], axis=0),
            wdt[...],
            preferred_element_type=jnp.float32,
        )
        for part_rows in (slice(0, half), slice(half, count))
    ]
    for slot in range(1, segs):
        for k, part_rows in enumerate((slice(0, half), slice(half, count))):
            hgrad[slot, part_rows] = halves[k][(slot - 1) * half : slot * half]
    for slot in range(1, segs):
        backward(slot)
    m_pair = put(mrow.at[0], mrow.at[1], across)
    for n, cols in enumerate(order):
        part[1:, :, cols] = (
            jnp.dot(
                back[1:].reshape(rest, 2 * feats),
                wgut[:, cols],
                preferred_element_type=jnp.float32,
            )
            .astype(jnp.bfloat16)
            .reshape(segs - 1, count, quarter)
        )
        swaps.append(
            [
                put(part.at[slot, theirs, cols], pin.at[slot, :, cols], across)
                for slot in (2, 3, 1)
            ]
        )
        if n == 1:
            m_pair.wait_recv()
            mrow[2] = mrow[0] + mrow[1]
            m_side = [
                put(mrow.at[2, slot], mland.at[slot - 1], target)
                for slot, target in ((1, Z), (2, X), (3, Y))
            ]
        if n >= 2:
            advance(n - 2)
    for n in range(depth - 2, depth):
        advance(n)

    def weight_step(n, carry):
        cols = pl.ds(pl.multiple_of(n * 512, 128), 512)
        block = contract_rows(rin[:, :, cols].reshape(segs * count, 512), back[...].reshape(segs * count, 2 * feats))
        gout[cols, :] = block[:, :feats].astype(jnp.bfloat16)
        uout[cols, :] = block[:, feats:].astype(jnp.bfloat16)
        return carry

    lax.fori_loop(0, width // 512, weight_step, 0)
    store(gout, gate_out)
    store(uout, up_out)

    def line_step(i, carry):
        q = pl.ds(pl.multiple_of(i * ROWS, ROWS), ROWS)
        r = pl.ds(pl.multiple_of(c * half + i * ROWS, ROWS), ROWS)
        total = part[1, r, span(z)].astype(jnp.float32)
        for k in range(depth - 1):
            total = total + rz1[k, q, :].astype(jnp.float32)
        sd[q, :] = total.astype(jnp.bfloat16)
        return carry

    swap_own.wait_recv()
    own_z = []
    for n, cols in enumerate(order):
        if n == depth - 1:
            for copy in d_z:
                copy.wait_recv()
            lax.fori_loop(0, line_rows // ROWS, line_step, 0)
            d_p = put(sd, rd, Z)
        for copies in (x_p, y_p, dd_p):
            copies[n].wait_recv()

        def step(i, carry):
            r = pl.ds(pl.multiple_of(c * half + i * ROWS, ROWS), ROWS)
            q = pl.ds(pl.multiple_of(i * ROWS, ROWS), ROWS)
            total = part[0, r, cols].astype(jnp.float32)
            for ref in (pin.at[0], rx, ry):
                total = total + ref[q, cols].astype(jnp.float32)
            part[0, r, cols] = total.astype(jnp.bfloat16)
            return carry

        def direct_step(i, carry):
            r = pl.ds(pl.multiple_of(c * half + i * ROWS, ROWS), ROWS)
            q = pl.ds(pl.multiple_of(i * ROWS, ROWS), ROWS)
            u = pl.ds(pl.multiple_of(i * ROWS - line_rows, ROWS), ROWS)
            total = part[0, r, cols].astype(jnp.float32)
            for ref in (pin.at[0], rx, ry):
                total = total + ref[q, cols].astype(jnp.float32)
            total = total + rdd[u, cols].astype(jnp.float32)
            part[0, r, cols] = total.astype(jnp.bfloat16)
            return carry

        lax.fori_loop(0, line_rows // ROWS, step, 0)
        lax.fori_loop(line_rows // ROWS, half // ROWS, direct_step, 0)
        if n == 0:
            total = mrow[2, 0]
            for k, copy in enumerate(m_side):
                copy.wait_recv()
                total = total + mland[k]
            msend[...] = total
            m_z = [put(msend, mz.at[i], along[i]) for i in range(depth - 1)]
        if n < depth - 1:
            own_z.append(put(part.at[0, mine, cols], rz2.at[n], along[n]))

    d_p.wait_recv()

    total = msend[...]
    for k, copy in enumerate(m_z):
        copy.wait_recv()
        total = total + mz[k]
    first = lax.broadcasted_iota(jnp.int32, (8, 128), 0) == 0
    means[...] = lax.dot_general(
        total / width, first.astype(jnp.float32), (((0,), (0,)), ((), ())), **exact
    )
    for copy in own_z:
        copy.wait_recv()

    def resid_step(i, u):
        q = pl.ds(pl.multiple_of(i * ROWS, ROWS), ROWS)
        r = pl.ds(pl.multiple_of(c * half + i * ROWS, ROWS), ROWS)
        total = part[0, r, span(z)].astype(jnp.float32)
        for k in range(depth - 1):
            total = total + rz2[k, q, :].astype(jnp.float32)
        if u is not None:
            total = total + rd[q, :].astype(jnp.float32)
        weighted = gain_ref[:, span(z)] * total
        inverse = inv[r, 0:1]
        scaled = raw_r[r, span(z)].astype(jnp.float32) * inverse
        grad = raw_o[r, span(z)].astype(jnp.float32) + inverse * (weighted - scaled * means[r, 0:1])
        rg[r, span(z)] = grad.astype(jnp.bfloat16)

    pieces = [(0, line_rows, True), (line_rows, half - line_rows, None)]
    g_z, g_f, col_copies = [], [], []

    def send_columns(k, q):
        for t, _, copy in col_copies[k]:

            @pl.when(q == t)
            def _():
                copy.start()

    def resid_piece(k):
        first_row, size, extra = pieces[k]

        def resid_loop(i, carry):
            resid_step(i, extra)
            return carry

        lax.fori_loop(first_row // ROWS, (first_row + size) // ROWS, resid_loop, 0)
        rows = pl.ds(pl.multiple_of(c * half + first_row, ROWS), size)
        block = rg.at[rows, span(z)]
        g_z.append(line_put(block))
        g_f.append([put(block, block, across)])
        col_copies.append(
            [
                (t, slot, remote(rg.at[rows, span(t)], col.at[slot, rows, :], target))
                for t, slot, target in ((gd, 1, Z), (gx, 2, X), (gy, 3, Y))
            ]
        )
        send_columns(k, z)

    resid_piece(0)
    def down_step(n, carry):
        cols = pl.ds(pl.multiple_of(n * 512, 128), 512)
        block = contract_rows(
            hid[...].reshape(segs * count, feats), og[:, :, cols].reshape(segs * count, 512)
        )
        dout[:, cols] = block.astype(jnp.bfloat16)
        return carry

    lax.fori_loop(0, width // 512, down_step, 0)
    store(dout, down_out)

    resid_piece(1)
    for slot, target in ((1, Z), (2, X), (3, Y)):
        extras.append(put(outs_all.at[0], outs_all.at[slot], target))
    load_op.wait()
    heads, col_f = [], []
    for k, (first_row, size, extra) in enumerate(pieces):
        rows = pl.ds(pl.multiple_of(c * half + first_row, ROWS), size)
        for i in range(depth - 1):
            g_z[k][i].wait_recv()
            block = rg.at[rows, span(downs[i])]
            g_f[k].append(put(block, block, across))
            send_columns(k, downs[i])
        for copy in g_f[k]:
            copy.wait_recv()
        spots = [slice(base + first_row, base + first_row + size) for base in (0, half)]
        lhs = jnp.concatenate([rg[spot, :] for spot in spots], axis=0)
        grads = contract_cols(lhs, op[...]).astype(jnp.bfloat16)
        for j, spot in enumerate(spots):
            hga[0, spot, :] = grads[j * size : (j + 1) * size]
        for spot in spots:
            for slot, target in ((1, Z), (2, X), (3, Y)):
                heads.append(put(hga.at[0, spot], hga.at[slot, spot], target))
    col[0] = rg[:, span(g)]
    for k, (first_row, size, extra) in enumerate(pieces):
        rows = pl.ds(pl.multiple_of(c * half + first_row, ROWS), size)
        for _, slot, copy in col_copies[k]:
            copy.wait_recv()
            block = col.at[slot, rows, :]
            col_f.append(put(block, block, across))
    for copy in extras:
        copy.wait_recv()
    store(outs_all, outs_out)
    store(fq_all, fq_out)
    store(ends_all, ends_out)
    for copy in col_f:
        copy.wait_recv()
    store(col, col_out)
    for copy in heads:
        copy.wait_recv()
    store(hga, hg_out)
    for copy in sends:
        copy.wait_send()
    for copy in stores:
        copy.wait()


def square_call(segs, raw_r, raw_o, ids, scale, decay, gain, wg, wu, wd, op, outs, query):
    count, width = raw_r.shape
    feats, heads = wg.shape[1], outs.shape[1]
    half, quarter = count // CORES, width // segs
    line = half * 3 // 5 // ROWS * ROWS
    bf16, f32 = jnp.bfloat16, jnp.float32
    any_spec = pl.BlockSpec(memory_space=pl.ANY)
    shape = jax.ShapeDtypeStruct
    flops = 2 * segs * count * width * feats * 8
    return pl.pallas_call(
        square_kernel,
        out_shape=(
            shape((width, feats), bf16),
            shape((width, feats), bf16),
            shape((feats, width), bf16),
            shape((segs, count, quarter), bf16),
            shape((segs, count, heads), bf16),
            shape((segs, count, heads), bf16),
            shape((segs, count, heads), bf16),
            shape((segs, 8, 128), f32),
        ),
        in_specs=[any_spec] * 12,
        out_specs=(any_spec,) * 8,
        scratch_shapes=[
            pltpu.VMEM(ids.shape, jnp.int32),
            pltpu.VMEM(scale.shape, f32),
            pltpu.VMEM(decay.shape, f32),
            pltpu.VMEM(gain.shape, f32),
            pltpu.VMEM((count, width), bf16),
            pltpu.VMEM((count, width), bf16),
            pltpu.VMEM((segs, count, width), bf16),
            pltpu.VMEM((segs, count, width), bf16),
            pltpu.VMEM((3, half, width), bf16),
            pltpu.VMEM((width, feats), bf16),
            pltpu.VMEM((width, feats), bf16),
            pltpu.VMEM((feats, width), bf16),
            pltpu.VMEM((width, feats), bf16),
            pltpu.VMEM((2 * feats, width), bf16),
            pltpu.VMEM((heads, width), bf16),
            pltpu.VMEM((segs, count, width), bf16),
            pltpu.VMEM((segs, half, width), bf16),
            pltpu.VMEM((segs, count, feats), bf16),
            pltpu.VMEM((segs, count, 2 * feats), bf16),
            pltpu.VMEM((segs, count, 2 * feats), f32),
            pltpu.VMEM((segs, count, feats), f32),
            pltpu.VMEM((segs, count, feats), f32),
            pltpu.VMEM((count, heads), bf16),
            pltpu.VMEM((half, width), bf16),
            pltpu.VMEM((half, width), bf16),
            pltpu.VMEM((half - line, width), bf16),
            pltpu.VMEM((segs - 1, line, quarter), bf16),
            pltpu.VMEM((line, quarter), bf16),
            pltpu.VMEM((line, quarter), bf16),
            pltpu.VMEM((segs - 1, half, quarter), bf16),
            pltpu.VMEM((count, 128), f32),
            pltpu.VMEM((count, 128), f32),
            pltpu.VMEM((count, 128), f32),
            pltpu.VMEM((3, segs, 8, count), f32),
            pltpu.VMEM((segs - 1, 8, count), f32),
            pltpu.VMEM((8, count), f32),
            pltpu.VMEM((segs - 1, 8, count), f32),
            pltpu.VMEM((count, width), bf16),
            pltpu.VMEM((segs, count, quarter), bf16),
            pltpu.VMEM((segs, count, heads), bf16),
            pltpu.VMEM((segs, count, heads), bf16),
            pltpu.VMEM((segs, count, heads), bf16),
            pltpu.VMEM((segs, 8, 128), f32),
            pltpu.VMEM((width, feats), bf16),
            pltpu.VMEM((width, feats), bf16),
            pltpu.VMEM((feats, width), bf16),
            pltpu.SemaphoreType.DMA((160,)),
            pltpu.SemaphoreType.DMA((160,)),
            pltpu.SemaphoreType.DMA((12,)),
            pltpu.SemaphoreType.DMA((8,)),
        ],
        compiler_params=pltpu.CompilerParams(
            collective_id=0, has_side_effects=True, vmem_limit_bytes=VMEM_LIMIT
        ),
        cost_estimate=pl.CostEstimate(flops=flops, bytes_accessed=40000000, transcendentals=0),
    )(raw_r, raw_o, ids, scale, decay, gain, wg, wu, wd, op, outs, query)


def tail_kernel(
    gate_in,
    up_in,
    down_in,
    col_hbm,
    hg_hbm,
    outs_hbm,
    fq_hbm,
    ends_hbm,
    query_hbm,
    key_hbm,
    value_hbm,
    entry_hbm,
    decay_hbm,
    gate_out,
    up_out,
    down_out,
    proj_out,
    query_out,
    key_out,
    value_out,
    gate,
    up,
    down,
    col,
    hga,
    outs,
    fqa,
    ends,
    query,
    key,
    value,
    entry,
    decay_ref,
    proj,
    query_grad,
    key_grad,
    value_grad,
    load_sems,
    store_sems,
):
    segs, count, quarter = col.shape
    heads_here = decay_ref.shape[0]
    head_width = query.shape[1] // heads_here
    channels = query.shape[1]
    loads = []

    def load(src, dst):
        copy = pltpu.make_async_copy(src, dst, load_sems.at[len(loads)])
        copy.start()
        loads.append(copy)
        return copy

    stores = []

    def store(src, dst):
        copy = pltpu.make_async_copy(src, dst, store_sems.at[len(stores)])
        copy.start()
        stores.append(copy)

    early = [
        load(*pair)
        for pair in (
            (decay_hbm, decay_ref),
            (query_hbm, query),
            (key_hbm, key),
            (value_hbm, value),
            (hg_hbm, hga),
            (fq_hbm, fqa),
            (ends_hbm, ends),
            (entry_hbm, entry),
        )
    ]
    load_col = [load(col_hbm, col), load(outs_hbm, outs)]
    through = [
        (load(gate_in, gate), gate, gate_out),
        (load(up_in, up), up, up_out),
        (load(down_in, down), down, down_out),
    ]
    g = lax.axis_index("sp")
    gy_, gx_ = g // 2, g % 2
    seg_of = [
        g,
        (1 - gy_) * 2 + (1 - gx_),
        gy_ * 2 + (1 - gx_),
        (1 - gy_) * 2 + gx_,
    ]
    row = lax.broadcasted_iota(jnp.int32, (count, count), 0)
    column = lax.broadcasted_iota(jnp.int32, (count, count), 1)
    causal = row >= column
    early[0].wait()
    decay = decay_ref[...]
    exact = dict(preferred_element_type=jnp.float32, precision=lax.Precision.HIGHEST)
    lower = causal.astype(jnp.float32)
    running = lax.dot_general(lower, decay, (((1,), (1,)), ((), ())), **exact)
    across = lax.dot_general(decay, lower, (((1,), (1,)), ((), ())), **exact)
    key_scale = head_width ** (-0.5)
    bf16 = jnp.bfloat16
    for copy in early[1:]:
        copy.wait()

    def mul(left, right):
        return jnp.dot(left, right, preferred_element_type=jnp.float32)

    for h in range(heads_here):
        cols = slice(h * head_width, (h + 1) * head_width)
        run = running[:, h : h + 1]
        from_start = jnp.exp(run)
        to_end = jnp.exp(running[count - 1 :, h : h + 1] - run)
        spread = jnp.where(causal, run - across[h : h + 1, :], 0.0)
        weights = jnp.where(causal, jnp.exp(spread), 0.0)
        state = jnp.zeros((head_width, head_width), jnp.float32)
        for j in range(1, segs):
            between = jnp.zeros((1, 1), jnp.float32)
            for i in range(1, segs):
                if i != j:
                    inside = (seg_of[i] > g) & (seg_of[i] < seg_of[j])
                    between = between + jnp.where(inside, ends[i, 0:1, h : h + 1], 0.0)
            passed = jnp.where(seg_of[j] > g, jnp.exp(between), 0.0)
            state = state + passed * contract_rows(fqa[j, :, cols], hga[j, :, cols])
        state = state.astype(bf16)
        grad = hga[0, :, cols]
        q, k, v = query[:, cols], key[:, cols], value[:, cols]
        grad_scores = (contract_cols(grad, v) * weights).astype(bf16)
        key_scores = (contract_cols(q, k) * weights).astype(bf16)
        query_grad[:, cols] = (
            key_scale
            * (mul(grad_scores, k) + from_start * contract_cols(grad, entry[h].astype(bf16)))
        ).astype(bf16)
        key_grad[:, cols] = (
            key_scale * (contract_rows(grad_scores, q) + to_end * contract_cols(v, state))
        ).astype(bf16)
        value_grad[:, cols] = (
            key_scale * (contract_rows(key_scores, grad) + to_end * mul(k, state))
        ).astype(bf16)
    store(query_grad, query_out)
    store(key_grad, key_out)
    store(value_grad, value_out)
    for copy, src, dst in through:
        copy.wait()
        store(src, dst)
    for copy in load_col:
        copy.wait()
    right = outs[...].reshape(segs * count, channels)
    for n in range(quarter // 256):
        cols = slice(n * 256, (n + 1) * 256)
        proj[cols, :] = contract_rows(col[:, :, cols].reshape(segs * count, 256), right)
        store(proj.at[cols, :], proj_out.at[cols, :])
    for copy in stores:
        copy.wait()


def tail_call(gate, up, down, col, hga, outs, fqa, ends, query, key, value, entry, decay):
    segs, count, quarter = col.shape
    channels = query.shape[1]
    any_spec = pl.BlockSpec(memory_space=pl.ANY)
    shape = jax.ShapeDtypeStruct
    rows = shape((count, channels), jnp.bfloat16)
    proj = shape((quarter, channels), jnp.float32)
    kept = [gate, up, down, col, hga, outs, fqa, ends, query, key, value, entry, decay]
    results = [proj, rows, rows, rows]
    return pl.pallas_call(
        tail_kernel,
        out_shape=tuple(shape(a.shape, a.dtype) for a in (gate, up, down)) + tuple(results),
        in_specs=[any_spec] * len(kept),
        out_specs=(any_spec,) * 7,
        scratch_shapes=[pltpu.VMEM(a.shape, a.dtype) for a in kept + results]
        + [pltpu.SemaphoreType.DMA((16,)), pltpu.SemaphoreType.DMA((16,))],
        compiler_params=pltpu.CompilerParams(vmem_limit_bytes=VMEM_LIMIT),
        cost_estimate=pl.CostEstimate(
            flops=2 * segs * count * quarter * channels,
            bytes_accessed=30000000,
            transcendentals=0,
        ),
    )(*kept)


def local_square(
    residual_mid,
    out_grad,
    norm_gain,
    expert_ids,
    expert_weights,
    gate_proj,
    up_proj,
    down_proj,
    out_proj,
    query_rows,
    key_rows,
    value_rows,
    retention_out,
    log_decay,
    entry_state,
):
    width = residual_mid.shape[1]
    segs = lax.axis_size("sp")
    gate_grad, up_grad, down_grad, columns, grads, outs, fqs, ends = square_call(
        segs,
        residual_mid,
        out_grad,
        expert_ids.T,
        expert_weights.T,
        log_decay.T,
        norm_gain.reshape(1, width),
        gate_proj[0],
        up_proj[0],
        down_proj[0],
        out_proj,
        retention_out,
        query_rows,
    )
    gate_grad, up_grad, down_grad, proj_grad, query_grad, key_grad, value_grad = tail_call(
        gate_grad,
        up_grad,
        down_grad,
        columns,
        grads,
        outs,
        fqs,
        ends,
        query_rows,
        key_rows,
        value_rows,
        entry_state[0],
        log_decay.T,
    )
    return (
        gate_grad[None],
        up_grad[None],
        down_grad[None],
        proj_grad,
        query_grad,
        key_grad,
        value_grad,
    )


def solution(mesh):
    segs, split = mesh.shape["sp"], mesh.shape["tp"]
    fine = Mesh(mesh.devices.reshape(segs, split // CORES, CORES), ("sp", "z", "core"))
    tp = ("z", "core")
    placed = (
        P("sp", None),
        P("sp", None),
        P(),
        P("sp", None),
        P("sp", None),
        P("sp", None, tp),
        P("sp", None, tp),
        P("sp", tp, None),
        P(tp, None),
        P("sp", tp),
        P("sp", tp),
        P("sp", tp),
        P("sp", tp),
        P("sp", tp),
        P("sp", tp, None, None),
    )
    fast = segs == 4 and split == segs * CORES
    return jax.shard_map(
        local_square if fast else local_general,
        mesh=fine,
        in_specs=placed,
        out_specs=(
            P("sp", None, tp),
            P("sp", None, tp),
            P("sp", tp, None),
            P("sp", tp),
            P("sp", tp),
            P("sp", tp),
            P("sp", tp),
        ),
        check_vma=False,
    )
```

```python
import jax
import jax.numpy as jnp
from jax import lax
from jax.experimental import pallas as pl
from jax.experimental.pallas import tpu as pltpu
from jax.sharding import Mesh, PartitionSpec as P

CLAMP_LIMIT = 7.0
GATE_ALPHA = 1.702
NORM_EPSILON = 1e-05
CORES = 2
SWAP = [(0, 1), (1, 0)]


def activate(gate_pre, up_pre):
    gate_clamped = jnp.minimum(gate_pre, CLAMP_LIMIT)
    up_clamped = jnp.clip(up_pre, -CLAMP_LIMIT, CLAMP_LIMIT)
    return (up_clamped + 1.0) * gate_clamped * jax.nn.sigmoid(GATE_ALPHA * gate_clamped)


def contract_rows(left, right):
    return lax.dot_general(
        left, right, (((0,), (0,)), ((), ())), preferred_element_type=jnp.float32
    )


def contract_cols(left, right):
    return lax.dot_general(
        left, right, (((1,), (1,)), ((), ())), preferred_element_type=jnp.float32
    )


def dots(spec, left, right):
    return jnp.einsum(
        spec,
        left.astype(jnp.bfloat16),
        right.astype(jnp.bfloat16),
        preferred_element_type=jnp.float32,
    )


def local_general(
    residual_mid,
    out_grad,
    norm_gain,
    expert_ids,
    expert_weights,
    gate_proj,
    up_proj,
    down_proj,
    out_proj,
    query_rows,
    key_rows,
    value_rows,
    retention_out,
    log_decay,
    entry_state,
):
    token_count, width = residual_mid.shape
    segs = lax.axis_size("sp")
    depth = lax.axis_size("z")
    seg = lax.axis_index("sp")
    core = lax.axis_index("core")
    half = token_count // CORES
    share = half // depth

    def rows_of(array, start, count):
        return lax.dynamic_slice_in_dim(array, start, count, axis=0)

    def normalize(rows):
        wide = rows.astype(jnp.float32)
        inverse = lax.rsqrt(jnp.mean(wide * wide, axis=1, keepdims=True) + NORM_EPSILON)
        return wide * inverse, inverse

    grad_own = lax.all_gather(rows_of(out_grad, core * half, half), "sp").reshape(-1, width)
    normed_half = (normalize(rows_of(residual_mid, core * half, half))[0] * norm_gain).astype(
        jnp.bfloat16
    )
    normed_own = lax.all_gather(normed_half, "sp").reshape(-1, width)
    grad_other = lax.ppermute(grad_own, "core", SWAP)
    normed_other = lax.ppermute(normed_own, "core", SWAP)

    experts = jnp.arange(segs, dtype=jnp.int32)
    route = jnp.sum(
        jnp.where(expert_ids.T[None] == experts[:, None, None], expert_weights.T[None], 0.0), axis=1
    )
    heads_here = log_decay.shape[1]
    small = jnp.concatenate([route.reshape(-1), jnp.sum(log_decay, axis=0)])
    smalls = lax.all_gather(small, "sp")
    routes = smalls[:, : segs * token_count].reshape(segs, segs, token_count)
    seg_decay = smalls[:, segs * token_count :]
    here = lax.dynamic_index_in_dim(routes, seg, axis=1, keepdims=False)
    here = here.reshape(segs, CORES, half)
    weight_own = lax.dynamic_index_in_dim(here, core, axis=1, keepdims=False).reshape(-1, 1)
    weight_other = lax.dynamic_index_in_dim(here, 1 - core, axis=1, keepdims=False).reshape(-1, 1)

    gate_weight = gate_proj[0]
    up_weight = up_proj[0]
    down_weight = down_proj[0]

    def expert(rows_in, rows_out, weight):
        rows_grad = (weight * rows_out.astype(jnp.float32)).astype(jnp.bfloat16)
        gate_pre = jnp.dot(rows_in, gate_weight, preferred_element_type=jnp.float32)
        up_pre = jnp.dot(rows_in, up_weight, preferred_element_type=jnp.float32)
        hidden, pullback = jax.vjp(activate, gate_pre, up_pre)
        gate_back, up_back = pullback(contract_cols(rows_grad, down_weight))
        gate_back = gate_back.astype(jnp.bfloat16)
        up_back = up_back.astype(jnp.bfloat16)
        part = contract_cols(gate_back, gate_weight) + contract_cols(up_back, up_weight)
        return part, rows_grad, hidden.astype(jnp.bfloat16), gate_back, up_back

    part_own, cot_own, hidden_own, gate_back_own, up_back_own = expert(
        normed_own, grad_own, weight_own
    )
    part_other, cot_other, hidden_other, gate_back_other, up_back_other = expert(
        normed_other, grad_other, weight_other
    )
    part_got = lax.ppermute(part_other.astype(jnp.bfloat16), "core", SWAP)
    part_pair = (part_own + part_got.astype(jnp.float32)).astype(jnp.bfloat16)
    part_seg = lax.psum_scatter(
        part_pair.reshape(segs, half, width), "sp", scatter_dimension=0, tiled=False
    )
    mixed_grad = lax.psum_scatter(
        part_seg.reshape(depth, share, width), "z", scatter_dimension=0, tiled=False
    ).astype(jnp.float32)

    down_grad = (contract_rows(hidden_own, cot_own) + contract_rows(hidden_other, cot_other)).astype(
        jnp.bfloat16
    )[None]
    gate_grad = (
        contract_rows(normed_own, gate_back_own) + contract_rows(normed_other, gate_back_other)
    ).astype(jnp.bfloat16)[None]
    up_grad = (
        contract_rows(normed_own, up_back_own) + contract_rows(normed_other, up_back_other)
    ).astype(jnp.bfloat16)[None]

    start = core * half + lax.axis_index("z") * share
    scaled, inverse = normalize(rows_of(residual_mid, start, share))
    weighted = norm_gain * mixed_grad
    inner = jnp.mean(scaled * weighted, axis=1, keepdims=True)
    resid_part = (
        rows_of(out_grad, start, share).astype(jnp.float32)
        + inverse * (weighted - scaled * inner)
    ).astype(jnp.bfloat16)
    resid_grad = lax.all_gather(resid_part, ("core", "z"), axis=0, tiled=False).reshape(
        token_count, width
    )
    columns = lax.all_to_all(
        resid_part.reshape(share, segs, width // segs).transpose(1, 0, 2),
        "sp",
        split_axis=0,
        concat_axis=0,
        tiled=True,
    )
    columns = lax.all_gather(columns, ("core", "z"), axis=0, tiled=False).reshape(
        segs * token_count, -1
    )
    outs = lax.all_gather(retention_out, "sp")
    outs = outs.reshape(segs, CORES * depth, share, -1).transpose(1, 0, 2, 3)
    outs = outs.reshape(segs * token_count, -1)
    proj_grad = contract_rows(columns, outs)

    head_grad = contract_cols(resid_grad, out_proj).astype(jnp.bfloat16)

    def split_heads(rows):
        return rows.reshape(token_count, heads_here, -1).transpose(1, 0, 2)

    queries = split_heads(query_rows)
    key_heads = split_heads(key_rows)
    value_heads = split_heads(value_rows)
    grad_heads = split_heads(head_grad)
    key_scale = queries.shape[2] ** (-0.5)
    running = jnp.cumsum(log_decay, axis=0).T
    from_start = jnp.exp(running)
    to_end = jnp.exp(running[:, -1:] - running)
    position = jnp.arange(token_count, dtype=jnp.int32)
    causal = (position[:, None] >= position[None, :])[None]
    spread = jnp.where(causal, running[:, :, None] - running[:, None, :], 0.0)
    weights = jnp.where(causal, jnp.exp(spread), 0.0)
    local_state = dots("htk,hte->hke", from_start[:, :, None] * queries, grad_heads)
    states = lax.all_gather(local_state.astype(jnp.bfloat16), "sp")
    order = jnp.arange(segs, dtype=jnp.int32)
    between = (order[None, :] > seg) & (order[None, :] < order[:, None])
    passed = jnp.exp(jnp.sum(jnp.where(between[:, :, None], seg_decay[None], 0.0), axis=1))
    passed = jnp.where(order[:, None] > seg, passed, 0.0)
    later_state = jnp.sum(passed[:, :, None, None] * states.astype(jnp.float32), axis=0)
    entry = entry_state[0]
    grad_scores = dots("hte,hse->hts", grad_heads, value_heads) * weights
    key_scores = dots("htk,hsk->hts", queries, key_heads) * weights
    query_grad = key_scale * (
        dots("hts,hsk->htk", grad_scores, key_heads)
        + from_start[:, :, None] * dots("hte,hke->htk", grad_heads, entry)
    )
    key_grad = key_scale * (
        dots("hts,htk->hsk", grad_scores, queries)
        + to_end[:, :, None] * dots("hse,hke->hsk", value_heads, later_state)
    )
    value_grad = key_scale * (
        dots("hts,hte->hse", key_scores, grad_heads)
        + to_end[:, :, None] * dots("hsk,hke->hse", key_heads, later_state)
    )

    def merge_heads(heads_rows):
        return heads_rows.transpose(1, 0, 2).reshape(token_count, -1).astype(jnp.bfloat16)

    return (
        gate_grad,
        up_grad,
        down_grad,
        proj_grad,
        merge_heads(query_grad),
        merge_heads(key_grad),
        merge_heads(value_grad),
    )


ROWS = 16
COPIES = 117
VMEM_LIMIT = 66 * 1000 * 1000
MESH_ID = pl.DeviceIdType.MESH


def square_kernel(
    raw_r_hbm,
    raw_o_hbm,
    ids_hbm,
    scale_hbm,
    decay_hbm,
    gain_hbm,
    wg_hbm,
    wu_hbm,
    wd_hbm,
    op_hbm,
    outs_hbm,
    query_hbm,
    gate_out,
    up_out,
    down_out,
    col_out,
    hg_out,
    outs_out,
    fq_out,
    ends_out,
    ids_ref,
    scale_ref,
    decay_ref,
    gain_ref,
    raw_r,
    raw_o,
    rin,
    og,
    stg,
    wg,
    wu,
    wd,
    wdt,
    wgut,
    op,
    part,
    pin,
    hid,
    back,
    pre,
    hgrad,
    slope_m,
    query,
    rx,
    ry,
    rdd,
    rz1,
    sd,
    rd,
    rz2,
    inv,
    route,
    means,
    mrow,
    mland,
    msend,
    mz,
    rg,
    col,
    hga,
    outs_all,
    fq_all,
    ends_all,
    gout,
    uout,
    dout,
    send_sems,
    recv_sems,
    load_sems,
    store_sems,
):
    segs, count, width = rin.shape
    half = count // CORES
    depth = segs
    quarter = width // depth
    feats = wg.shape[1]
    g = lax.axis_index("sp")
    z = lax.axis_index("z")
    c = lax.axis_index("core")
    gy_, gx_ = g // 2, g % 2
    gx = gy_ * 2 + (1 - gx_)
    gy = (1 - gy_) * 2 + gx_
    gd = (1 - gy_) * 2 + (1 - gx_)
    ups = [(z + i) % depth for i in range(1, depth)]
    downs = [(z + depth - i) % depth for i in range(1, depth)]
    mine = pl.ds(pl.multiple_of(c * half, ROWS), half)
    theirs = pl.ds(pl.multiple_of((1 - c) * half, ROWS), half)

    def span(index):
        return pl.ds(pl.multiple_of(index * quarter, 128), quarter)

    def dev(sp, zz, cc):
        return {"sp": sp, "z": zz, "core": cc}

    sends = []
    used = [0]

    def remote(src, dst, target):
        k = used[0]
        used[0] += 1
        copy = pltpu.make_async_remote_copy(
            src_ref=src,
            dst_ref=dst,
            send_sem=send_sems.at[k],
            recv_sem=recv_sems.at[k],
            device_id=target,
            device_id_type=MESH_ID,
        )
        sends.append(copy)
        return copy

    def put(src, dst, target):
        copy = remote(src, dst, target)
        copy.start()
        return copy

    def line_put(block):
        return [put(block, block, target) for target in along]

    loads = []

    def load(src, dst):
        copy = pltpu.make_async_copy(src, dst, load_sems.at[len(loads)])
        copy.start()
        loads.append(copy)
        return copy

    stores = []

    def store(src, dst):
        copy = pltpu.make_async_copy(src, dst, store_sems.at[len(stores)])
        copy.start()
        stores.append(copy)

    load_small = [load(ids_hbm, ids_ref), load(scale_hbm, scale_ref)]
    load_gain = load(gain_hbm, gain_ref)
    load_r = load(raw_r_hbm, raw_r)
    load_o = load(raw_o_hbm, raw_o)
    load_decay = load(decay_hbm, decay_ref)
    load_w = [load(wg_hbm, wg), load(wu_hbm, wu), load(wd_hbm, wd)]
    load_op = load(op_hbm, op)
    load_outs = load(outs_hbm, outs_all.at[0])
    load_query = load(query_hbm, query)

    X, Y, Z = dev(gx, z, c), dev(gy, z, c), dev(gd, z, c)
    across = dev(g, z, 1 - c)
    along = [dev(g, zz, c) for zz in ups]
    barrier = pltpu.get_barrier_semaphore()
    for target in [X, Y, Z, across] + along:
        pl.semaphore_signal(barrier, inc=1, device_id=target, device_id_type=MESH_ID)

    kinds = (g, gd, gx, gy)
    which = lax.broadcasted_iota(jnp.int32, (8, count), 0)
    for copy in load_small:
        copy.wait()
    table = jnp.zeros((8, count), jnp.float32)
    for k, expert in enumerate(kinds):
        chosen = jnp.where(ids_ref[...] == expert, scale_ref[...], 0.0)
        table = jnp.where(which == k, jnp.sum(chosen, axis=0, keepdims=True), table)
    unit = lax.broadcasted_iota(jnp.int32, (8, 128), 0) == lax.broadcasted_iota(
        jnp.int32, (8, 128), 1
    )
    exact = dict(preferred_element_type=jnp.float32, precision=lax.Precision.HIGHEST)
    route[...] = lax.dot_general(
        table, unit.astype(jnp.float32), (((0,), (0,)), ((), ())), **exact
    )

    def weigh(base, rows, kind, write):
        def step(i, carry):
            r = pl.ds(pl.multiple_of(base + i * ROWS, ROWS), ROWS)
            w = route[r, kind : kind + 1]
            write(i, r, (w * raw_o[r, :].astype(jnp.float32)).astype(jnp.bfloat16))
            return carry

        lax.fori_loop(0, rows // ROWS, step, 0)

    def stage(index):
        def write(i, r, value):
            stg[index, pl.ds(pl.multiple_of(i * ROWS, ROWS), ROWS), :] = value

        return write

    def own_write(i, r, value):
        og[0, r, :] = value

    def normalize(base, rows):
        def step(i, carry):
            r = pl.ds(pl.multiple_of(base + i * ROWS, ROWS), ROWS)
            wide = raw_r[r, :].astype(jnp.float32)
            inverse = lax.rsqrt(jnp.mean(wide * wide, axis=1, keepdims=True) + NORM_EPSILON)
            inv[r, :] = jnp.broadcast_to(inverse, (ROWS, 128))
            rin[0, r, :] = (wide * inverse * gain_ref[...]).astype(jnp.bfloat16)
            return carry

        lax.fori_loop(0, rows // ROWS, step, 0)

    load_gain.wait()
    load_r.wait()
    normalize(c * half, half)
    pl.semaphore_wait(barrier, 4 + len(along))
    d_n = put(rin.at[0, mine, span(z)], rin.at[1, mine, span(z)], Z)
    load_o.wait()
    weigh(c * half, half, 1, stage(2))
    d_o = put(stg.at[2, :, span(z)], og.at[1, mine, span(z)], Z)
    x_n = put(rin.at[0, mine, :], rin.at[2, mine, :], X)
    y_n = put(rin.at[0, mine, :], rin.at[3, mine, :], Y)
    weigh(c * half, half, 2, stage(0))
    line_rows = rz1.shape[1]
    cuts = [(0, line_rows), (line_rows, half - line_rows)]

    def rows_of(cut):
        return pl.ds(pl.multiple_of(c * half + cut[0], ROWS), cut[1])

    def send_cut(index, slot, target, cut):
        return put(stg.at[index, slice(cut[0], cut[0] + cut[1]), :], og.at[slot, rows_of(cut), :], target)

    x_o = [send_cut(0, 2, X, cut) for cut in cuts]
    weigh(c * half, half, 3, stage(1))
    y_o = [send_cut(1, 3, Y, cut) for cut in cuts]

    def spread(buf):
        block = buf.at[1, mine, span(z)]
        return line_put(block) + [put(block, block, across)]

    def collect(buf, copies, i):
        copies[i].wait_recv()
        block = buf.at[1, mine, span(downs[i])]
        return put(block, block, across)

    def forward(buf, slot):
        block = buf.at[slot, mine, :]
        return put(block, block, across)

    d_n.wait_recv()
    n_spread = spread(rin)
    normalize((1 - c) * half, half)
    weigh(0, count, 0, own_write)
    d_o.wait_recv()
    o_spread = spread(og)

    load_decay.wait()
    heads_here = decay_ref.shape[0]
    head_width = query.shape[1] // heads_here
    later = lax.broadcasted_iota(jnp.int32, (count, count), 0)
    lower = (later >= lax.broadcasted_iota(jnp.int32, (count, count), 1)).astype(jnp.float32)
    running = lax.dot_general(lower, decay_ref[...], (((1,), (1,)), ((), ())), **exact)
    load_query.wait()
    for h in range(heads_here):
        cols = slice(h * head_width, (h + 1) * head_width)
        fq_all[0, :, cols] = (
            jnp.exp(running[:, h : h + 1]) * query[:, cols].astype(jnp.float32)
        ).astype(jnp.bfloat16)
    ends_all[0] = jnp.zeros((8, 128), jnp.float32)
    ends_all[0, :, :heads_here] = jnp.broadcast_to(running[count - 1 :, :], (8, heads_here))
    load_outs.wait()
    extras = []
    for slot, target in ((2, X), (3, Y), (1, Z)):
        extras.append(put(ends_all.at[0], ends_all.at[slot], target))
    shared = [put(fq_all.at[0], fq_all.at[slot], target) for slot, target in ((2, X), (3, Y))]

    for copy in load_w:
        copy.wait()

    def gates(slots, rows):
        lhs = rin[slots].reshape(rows, width)
        pre[slots, :, :feats] = jnp.dot(
            lhs, wg[...], preferred_element_type=jnp.float32
        ).reshape(-1, count, feats)
        pre[slots, :, feats:] = jnp.dot(
            lhs, wu[...], preferred_element_type=jnp.float32
        ).reshape(-1, count, feats)

    def slopes(s):
        gate_pre, up_pre = pre[s, :, :feats], pre[s, :, feats:]
        hidden, pullback = jax.vjp(activate, gate_pre, up_pre)
        gate_slope, up_slope = pullback(jnp.ones_like(hidden))
        hid[s] = hidden.astype(jnp.bfloat16)
        slope_m[s] = gate_slope * gate_pre + up_slope * up_pre
        pre[s, :, :feats] = gate_slope
        pre[s, :, feats:] = up_slope

    def backward(s):
        grad = hgrad[s]
        mrow[0, s] = lax.dot_general(
            jnp.ones((8, feats), jnp.float32),
            grad * slope_m[s],
            (((1,), (1,)), ((), ())),
            **exact,
        )
        back[s, :, :feats] = (grad * pre[s, :, :feats]).astype(jnp.bfloat16)
        back[s, :, feats:] = (grad * pre[s, :, feats:]).astype(jnp.bfloat16)

    def pair_step(s, cols):
        def step(i, carry):
            r = pl.ds(pl.multiple_of(c * half + i * ROWS, ROWS), ROWS)
            q = pl.ds(pl.multiple_of(i * ROWS, ROWS), ROWS)
            total = part[s, r, cols].astype(jnp.float32) + pin[s, q, cols].astype(jnp.float32)
            part[s, r, cols] = total.astype(jnp.bfloat16)
            return carry

        lax.fori_loop(0, half // ROWS, step, 0)

    gates(slice(0, 1), count)
    slopes(0)
    hgrad[0] = contract_cols(og[0], wd[...])
    backward(0)

    def own_step(n, carry):
        cols = span(n)
        piece = contract_cols(back[0, :, :feats], wg[cols, :]) + contract_cols(
            back[0, :, feats:], wu[cols, :]
        )
        part[0, :, cols] = piece.astype(jnp.bfloat16)
        return carry

    lax.fori_loop(0, depth, own_step, 0)
    swap_own = put(part.at[0, theirs, :], pin.at[0], across)


    def turn(n, carry):
        cols = pl.ds(pl.multiple_of(n * 512, 128), 512)
        wdt[cols, :] = wd[:, cols].T
        wgut[:feats, cols] = wg[cols, :].T
        wgut[feats:, cols] = wu[cols, :].T
        return carry

    lax.fori_loop(0, width // 512, turn, 0)
    rest = (segs - 1) * count
    x_n.wait_recv()
    f = [forward(rin, 2)]
    y_n.wait_recv()
    f.append(forward(rin, 3))
    for i in range(depth - 1):
        f.append(collect(rin, n_spread, i))
    n_spread[-1].wait_recv()
    for copy in f:
        copy.wait_recv()
    gates(slice(1, segs), rest)
    for slot in range(1, segs):
        slopes(slot)
    f = []
    for i in range(depth - 1):
        f.append(collect(og, o_spread, i))
    for k, cut in enumerate(cuts):
        for slot, copies in ((2, x_o), (3, y_o)):
            copies[k].wait_recv()
            block = og.at[slot, rows_of(cut), :]
            f.append(put(block, block, across))
    o_spread[-1].wait_recv()
    for copy in f:
        copy.wait_recv()

    def pair(s, swap, extra=()):
        swap.wait_recv()

        def step(i, carry):
            r = pl.ds(pl.multiple_of(c * half + i * ROWS, ROWS), ROWS)
            q = pl.ds(pl.multiple_of(i * ROWS, ROWS), ROWS)
            total = part[s, r, :].astype(jnp.float32) + pin[s, q, :].astype(jnp.float32)
            for ref in extra:
                total = total + ref[q, :].astype(jnp.float32)
            part[s, r, :] = total.astype(jnp.bfloat16)
            return carry

        lax.fori_loop(0, half // ROWS, step, 0)

    on_line = pl.ds(pl.multiple_of(c * half, ROWS), line_rows)
    direct = pl.ds(pl.multiple_of(c * half + line_rows, ROWS), half - line_rows)
    order = [span(q) for q in ups] + [span(z)]
    swaps, x_p, y_p, dd_p, d_z = [], [], [], [], []

    def advance(n):
        cols = order[n]
        swaps[n].wait_recv()
        pair_step(2, cols)
        x_p.append(put(part.at[2, mine, cols], rx.at[:, cols], X))
        pair_step(3, cols)
        y_p.append(put(part.at[3, mine, cols], ry.at[:, cols], Y))
        pair_step(1, cols)
        dd_p.append(put(part.at[1, direct, cols], rdd.at[:, cols], Z))
        if n < depth - 1:
            d_z.append(put(part.at[1, on_line, cols], rz1.at[n], along[n]))

    halves = [
        jnp.dot(
            jnp.concatenate([og[1, part_rows], og[2, part_rows], og[3, part_rows]], axis=0),
            wdt[...],
            preferred_element_type=jnp.float32,
        )
        for part_rows in (slice(0, half), slice(half, count))
    ]
    for slot in range(1, segs):
        for k, part_rows in enumerate((slice(0, half), slice(half, count))):
            hgrad[slot, part_rows] = halves[k][(slot - 1) * half : slot * half]
    for slot in range(1, segs):
        backward(slot)
    m_pair = put(mrow.at[0], mrow.at[1], across)
    for n, cols in enumerate(order):
        part[1:, :, cols] = (
            jnp.dot(
                back[1:].reshape(rest, 2 * feats),
                wgut[:, cols],
                preferred_element_type=jnp.float32,
            )
            .astype(jnp.bfloat16)
            .reshape(segs - 1, count, quarter)
        )
        others = pl.ds(1, segs - 1)
        swaps.append(put(part.at[others, theirs, cols], pin.at[others, :, cols], across))
        if n == 1:
            m_pair.wait_recv()
            mrow[2] = mrow[0] + mrow[1]
            m_side = [
                put(mrow.at[2, slot], mland.at[slot - 1], target)
                for slot, target in ((1, Z), (2, X), (3, Y))
            ]
        if n >= 2:
            advance(n - 2)
    for n in range(depth - 2, depth):
        advance(n)

    def weight_step(n, carry):
        cols = pl.ds(pl.multiple_of(n * 512, 128), 512)
        block = contract_rows(rin[:, :, cols].reshape(segs * count, 512), back[...].reshape(segs * count, 2 * feats))
        gout[cols, :] = block[:, :feats].astype(jnp.bfloat16)
        uout[cols, :] = block[:, feats:].astype(jnp.bfloat16)
        return carry

    lax.fori_loop(0, width // 512, weight_step, 0)
    store(gout, gate_out)
    store(uout, up_out)

    def line_step(i, carry):
        q = pl.ds(pl.multiple_of(i * ROWS, ROWS), ROWS)
        r = pl.ds(pl.multiple_of(c * half + i * ROWS, ROWS), ROWS)
        total = part[1, r, span(z)].astype(jnp.float32)
        for k in range(depth - 1):
            total = total + rz1[k, q, :].astype(jnp.float32)
        sd[q, :] = total.astype(jnp.bfloat16)
        return carry

    swap_own.wait_recv()
    own_z = []
    for n, cols in enumerate(order):
        if n == depth - 1:
            for copy in d_z:
                copy.wait_recv()
            lax.fori_loop(0, line_rows // ROWS, line_step, 0)
            d_p = put(sd, rd, Z)
        for copies in (x_p, y_p, dd_p):
            copies[n].wait_recv()

        def step(i, carry):
            r = pl.ds(pl.multiple_of(c * half + i * ROWS, ROWS), ROWS)
            q = pl.ds(pl.multiple_of(i * ROWS, ROWS), ROWS)
            total = part[0, r, cols].astype(jnp.float32)
            for ref in (pin.at[0], rx, ry):
                total = total + ref[q, cols].astype(jnp.float32)
            part[0, r, cols] = total.astype(jnp.bfloat16)
            return carry

        def direct_step(i, carry):
            r = pl.ds(pl.multiple_of(c * half + i * ROWS, ROWS), ROWS)
            q = pl.ds(pl.multiple_of(i * ROWS, ROWS), ROWS)
            u = pl.ds(pl.multiple_of(i * ROWS - line_rows, ROWS), ROWS)
            total = part[0, r, cols].astype(jnp.float32)
            for ref in (pin.at[0], rx, ry):
                total = total + ref[q, cols].astype(jnp.float32)
            total = total + rdd[u, cols].astype(jnp.float32)
            part[0, r, cols] = total.astype(jnp.bfloat16)
            return carry

        lax.fori_loop(0, line_rows // ROWS, step, 0)
        lax.fori_loop(line_rows // ROWS, half // ROWS, direct_step, 0)
        if n == 0:
            total = mrow[2, 0]
            for k, copy in enumerate(m_side):
                copy.wait_recv()
                total = total + mland[k]
            msend[...] = total
            m_z = [put(msend, mz.at[i], along[i]) for i in range(depth - 1)]
        if n < depth - 1:
            own_z.append(put(part.at[0, mine, cols], rz2.at[n], along[n]))

    d_p.wait_recv()

    total = msend[...]
    for k, copy in enumerate(m_z):
        copy.wait_recv()
        total = total + mz[k]
    first = lax.broadcasted_iota(jnp.int32, (8, 128), 0) == 0
    means[...] = lax.dot_general(
        total / width, first.astype(jnp.float32), (((0,), (0,)), ((), ())), **exact
    )
    for copy in own_z:
        copy.wait_recv()

    def resid_step(i, u):
        q = pl.ds(pl.multiple_of(i * ROWS, ROWS), ROWS)
        r = pl.ds(pl.multiple_of(c * half + i * ROWS, ROWS), ROWS)
        total = part[0, r, span(z)].astype(jnp.float32)
        for k in range(depth - 1):
            total = total + rz2[k, q, :].astype(jnp.float32)
        if u is not None:
            total = total + rd[q, :].astype(jnp.float32)
        weighted = gain_ref[:, span(z)] * total
        inverse = inv[r, 0:1]
        scaled = raw_r[r, span(z)].astype(jnp.float32) * inverse
        grad = raw_o[r, span(z)].astype(jnp.float32) + inverse * (weighted - scaled * means[r, 0:1])
        rg[r, span(z)] = grad.astype(jnp.bfloat16)

    pieces = []
    while sum(size for _, size in pieces) < half:
        first_row = sum(size for _, size in pieces)
        pieces.append((first_row, min(2 * ROWS, half - first_row)))
    g_z, g_f, col_copies = [], [], []

    def send_columns(k, q):
        for t, _, copy in col_copies[k]:

            @pl.when(q == t)
            def _():
                copy.start()

    def resid_line(i, carry):
        resid_step(i, True)
        return carry

    def resid_direct(i, carry):
        resid_step(i, None)
        return carry

    lax.fori_loop(0, line_rows // ROWS, resid_line, 0)
    lax.fori_loop(line_rows // ROWS, half // ROWS, resid_direct, 0)

    def resid_piece(k):
        first_row, size = pieces[k]
        rows = pl.ds(pl.multiple_of(c * half + first_row, ROWS), size)
        block = rg.at[rows, span(z)]
        g_z.append(line_put(block))
        g_f.append([put(block, block, across)])
        col_copies.append(
            [
                (t, slot, remote(rg.at[rows, span(t)], col.at[slot, rows, :], target))
                for t, slot, target in ((gd, 1, Z), (gx, 2, X), (gy, 3, Y))
            ]
        )
        send_columns(k, z)

    resid_piece(0)
    for slot, target in ((2, X), (3, Y), (1, Z)):
        extras.append(put(outs_all.at[0], outs_all.at[slot], target))
    for k, (rows, target) in enumerate(((slice(0, half), Y), (slice(half, count), X))):
        shared[k].wait_recv()
        extras.append(put(fq_all.at[2 + k, rows], fq_all.at[1, rows], target))
    def down_step(n, carry):
        cols = pl.ds(pl.multiple_of(n * 512, 128), 512)
        block = contract_rows(
            hid[...].reshape(segs * count, feats), og[:, :, cols].reshape(segs * count, 512)
        )
        dout[:, cols] = block.astype(jnp.bfloat16)
        return carry

    lax.fori_loop(0, width // 512, down_step, 0)
    store(dout, down_out)

    resid_piece(1)
    load_op.wait()

    def turn_op(n, carry):
        cols = pl.ds(pl.multiple_of(n * 512, 128), 512)
        wg[cols, :] = op[:feats, cols].T
        wu[cols, :] = op[feats:, cols].T
        return carry

    lax.fori_loop(0, width // 512, turn_op, 0)
    heads, col_f = [], []
    for k, (first_row, size) in enumerate(pieces):
        rows = pl.ds(pl.multiple_of(c * half + first_row, ROWS), size)
        for i in range(depth - 1):
            g_z[k][i].wait_recv()
            block = rg.at[rows, span(downs[i])]
            g_f[k].append(put(block, block, across))
            send_columns(k, downs[i])
        if k + 2 < len(pieces):
            resid_piece(k + 2)
        for copy in g_f[k]:
            copy.wait_recv()
        spot = slice(first_row, first_row + size)
        lhs = jnp.concatenate(
            [rg[base + first_row : base + first_row + size, :] for base in (0, half)], axis=0
        )
        for k, turned in enumerate((wg, wu)):
            grads = jnp.dot(lhs, turned[...], preferred_element_type=jnp.float32)
            grads = grads.astype(jnp.bfloat16)
            for j in range(CORES):
                hga[0, j, spot, k * feats : (k + 1) * feats] = grads[j * size : (j + 1) * size]
        for slot, target in ((1, Z), (2, X), (3, Y)):
            heads.append(put(hga.at[0, :, spot], hga.at[slot, :, spot], target))
    col[0] = rg[:, span(g)]
    for k, (first_row, size) in enumerate(pieces):
        rows = pl.ds(pl.multiple_of(c * half + first_row, ROWS), size)
        for _, slot, copy in col_copies[k]:
            copy.wait_recv()
            block = col.at[slot, rows, :]
            col_f.append(put(block, block, across))
    for copy in extras:
        copy.wait_recv()
    store(outs_all, outs_out)
    store(fq_all, fq_out)
    store(ends_all, ends_out)
    for copy in col_f:
        copy.wait_recv()
    store(col, col_out)
    for copy in heads:
        copy.wait_recv()
    store(hga, hg_out)
    for copy in sends:
        copy.wait_send()
    for copy in stores:
        copy.wait()


def square_call(segs, raw_r, raw_o, ids, scale, decay, gain, wg, wu, wd, op, outs, query):
    count, width = raw_r.shape
    feats, heads = wg.shape[1], outs.shape[1]
    half, quarter = count // CORES, width // segs
    line = half * 3 // 5 // ROWS * ROWS
    bf16, f32 = jnp.bfloat16, jnp.float32
    any_spec = pl.BlockSpec(memory_space=pl.ANY)
    shape = jax.ShapeDtypeStruct
    flops = 2 * segs * count * width * feats * 8
    return pl.pallas_call(
        square_kernel,
        out_shape=(
            shape((width, feats), bf16),
            shape((width, feats), bf16),
            shape((feats, width), bf16),
            shape((segs, count, quarter), bf16),
            shape((segs, CORES, half, heads), bf16),
            shape((segs, count, heads), bf16),
            shape((segs, count, heads), bf16),
            shape((segs, 8, 128), f32),
        ),
        in_specs=[any_spec] * 12,
        out_specs=(any_spec,) * 8,
        scratch_shapes=[
            pltpu.VMEM(ids.shape, jnp.int32),
            pltpu.VMEM(scale.shape, f32),
            pltpu.VMEM(decay.shape, f32),
            pltpu.VMEM(gain.shape, f32),
            pltpu.VMEM((count, width), bf16),
            pltpu.VMEM((count, width), bf16),
            pltpu.VMEM((segs, count, width), bf16),
            pltpu.VMEM((segs, count, width), bf16),
            pltpu.VMEM((3, half, width), bf16),
            pltpu.VMEM((width, feats), bf16),
            pltpu.VMEM((width, feats), bf16),
            pltpu.VMEM((feats, width), bf16),
            pltpu.VMEM((width, feats), bf16),
            pltpu.VMEM((2 * feats, width), bf16),
            pltpu.VMEM((heads, width), bf16),
            pltpu.VMEM((segs, count, width), bf16),
            pltpu.VMEM((segs, half, width), bf16),
            pltpu.VMEM((segs, count, feats), bf16),
            pltpu.VMEM((segs, count, 2 * feats), bf16),
            pltpu.VMEM((segs, count, 2 * feats), f32),
            pltpu.VMEM((segs, count, feats), f32),
            pltpu.VMEM((segs, count, feats), f32),
            pltpu.VMEM((count, heads), bf16),
            pltpu.VMEM((half, width), bf16),
            pltpu.VMEM((half, width), bf16),
            pltpu.VMEM((half - line, width), bf16),
            pltpu.VMEM((segs - 1, line, quarter), bf16),
            pltpu.VMEM((line, quarter), bf16),
            pltpu.VMEM((line, quarter), bf16),
            pltpu.VMEM((segs - 1, half, quarter), bf16),
            pltpu.VMEM((count, 128), f32),
            pltpu.VMEM((count, 128), f32),
            pltpu.VMEM((count, 128), f32),
            pltpu.VMEM((3, segs, 8, count), f32),
            pltpu.VMEM((segs - 1, 8, count), f32),
            pltpu.VMEM((8, count), f32),
            pltpu.VMEM((segs - 1, 8, count), f32),
            pltpu.VMEM((count, width), bf16),
            pltpu.VMEM((segs, count, quarter), bf16),
            pltpu.VMEM((segs, CORES, half, heads), bf16),
            pltpu.VMEM((segs, count, heads), bf16),
            pltpu.VMEM((segs, count, heads), bf16),
            pltpu.VMEM((segs, 8, 128), f32),
            pltpu.VMEM((width, feats), bf16),
            pltpu.VMEM((width, feats), bf16),
            pltpu.VMEM((feats, width), bf16),
            pltpu.SemaphoreType.DMA((COPIES,)),
            pltpu.SemaphoreType.DMA((COPIES,)),
            pltpu.SemaphoreType.DMA((12,)),
            pltpu.SemaphoreType.DMA((8,)),
        ],
        compiler_params=pltpu.CompilerParams(
            collective_id=0, has_side_effects=True, vmem_limit_bytes=VMEM_LIMIT
        ),
        cost_estimate=pl.CostEstimate(flops=flops, bytes_accessed=40000000, transcendentals=0),
    )(raw_r, raw_o, ids, scale, decay, gain, wg, wu, wd, op, outs, query)


def tail_kernel(
    gate_in,
    up_in,
    down_in,
    col_hbm,
    hg_hbm,
    outs_hbm,
    fq_hbm,
    ends_hbm,
    query_hbm,
    key_hbm,
    value_hbm,
    entry_hbm,
    decay_hbm,
    gate_out,
    up_out,
    down_out,
    proj_out,
    query_out,
    key_out,
    value_out,
    gate,
    up,
    down,
    col,
    hga,
    outs,
    fqa,
    ends,
    query,
    key,
    value,
    entry,
    decay_ref,
    proj,
    query_grad,
    key_grad,
    value_grad,
    load_sems,
    store_sems,
):
    segs, count, quarter = col.shape
    heads_here = decay_ref.shape[0]
    head_width = query.shape[1] // heads_here
    channels = query.shape[1]
    loads = []

    def load(src, dst):
        copy = pltpu.make_async_copy(src, dst, load_sems.at[len(loads)])
        copy.start()
        loads.append(copy)
        return copy

    stores = []

    def store(src, dst):
        copy = pltpu.make_async_copy(src, dst, store_sems.at[len(stores)])
        copy.start()
        stores.append(copy)

    early = [
        load(*pair)
        for pair in (
            (decay_hbm, decay_ref),
            (query_hbm, query),
            (key_hbm, key),
            (value_hbm, value),
            (hg_hbm, hga),
            (fq_hbm, fqa),
            (ends_hbm, ends),
            (entry_hbm, entry),
        )
    ]
    load_col = [load(col_hbm, col), load(outs_hbm, outs)]
    through = [
        (load(gate_in, gate), gate, gate_out),
        (load(up_in, up), up, up_out),
        (load(down_in, down), down, down_out),
    ]
    g = lax.axis_index("sp")
    gy_, gx_ = g // 2, g % 2
    seg_of = [
        g,
        (1 - gy_) * 2 + (1 - gx_),
        gy_ * 2 + (1 - gx_),
        (1 - gy_) * 2 + gx_,
    ]
    row = lax.broadcasted_iota(jnp.int32, (count, count), 0)
    column = lax.broadcasted_iota(jnp.int32, (count, count), 1)
    causal = row >= column
    early[0].wait()
    decay = decay_ref[...]
    exact = dict(preferred_element_type=jnp.float32, precision=lax.Precision.HIGHEST)
    lower = causal.astype(jnp.float32)
    running = lax.dot_general(lower, decay, (((1,), (1,)), ((), ())), **exact)
    across = lax.dot_general(decay, lower, (((1,), (1,)), ((), ())), **exact)
    key_scale = head_width ** (-0.5)
    bf16 = jnp.bfloat16
    for copy in early[1:]:
        copy.wait()

    def mul(left, right):
        return jnp.dot(left, right, preferred_element_type=jnp.float32)

    for h in range(heads_here):
        cols = slice(h * head_width, (h + 1) * head_width)
        run = running[:, h : h + 1]
        from_start = jnp.exp(run)
        to_end = jnp.exp(running[count - 1 :, h : h + 1] - run)
        spread = jnp.where(causal, run - across[h : h + 1, :], 0.0)
        weights = jnp.where(causal, jnp.exp(spread), 0.0)
        state = jnp.zeros((head_width, head_width), jnp.float32)
        for j in range(1, segs):
            between = jnp.zeros((1, 1), jnp.float32)
            for i in range(1, segs):
                if i != j:
                    inside = (seg_of[i] > g) & (seg_of[i] < seg_of[j])
                    between = between + jnp.where(inside, ends[i, 0:1, h : h + 1], 0.0)
            passed = jnp.where(seg_of[j] > g, jnp.exp(between), 0.0)
            state = state + passed * contract_rows(fqa[j, :, cols], hga[j, :, cols])
        state = state.astype(bf16)
        grad = hga[0, :, cols]
        q, k, v = query[:, cols], key[:, cols], value[:, cols]
        grad_scores = (contract_cols(grad, v) * weights).astype(bf16)
        key_scores = (contract_cols(q, k) * weights).astype(bf16)
        query_grad[:, cols] = (
            key_scale
            * (mul(grad_scores, k) + from_start * contract_cols(grad, entry[h].astype(bf16)))
        ).astype(bf16)
        key_grad[:, cols] = (
            key_scale * (contract_rows(grad_scores, q) + to_end * contract_cols(v, state))
        ).astype(bf16)
        value_grad[:, cols] = (
            key_scale * (contract_rows(key_scores, grad) + to_end * mul(k, state))
        ).astype(bf16)
    store(query_grad, query_out)
    store(key_grad, key_out)
    store(value_grad, value_out)
    for copy, src, dst in through:
        copy.wait()
        store(src, dst)
    for copy in load_col:
        copy.wait()
    right = outs[...].reshape(segs * count, channels)
    for n in range(quarter // 256):
        cols = slice(n * 256, (n + 1) * 256)
        proj[cols, :] = contract_rows(col[:, :, cols].reshape(segs * count, 256), right)
        store(proj.at[cols, :], proj_out.at[cols, :])
    for copy in stores:
        copy.wait()


def tail_call(gate, up, down, col, hga, outs, fqa, ends, query, key, value, entry, decay):
    segs, count, quarter = col.shape
    channels = query.shape[1]
    any_spec = pl.BlockSpec(memory_space=pl.ANY)
    shape = jax.ShapeDtypeStruct
    rows = shape((count, channels), jnp.bfloat16)
    proj = shape((quarter, channels), jnp.float32)
    kept = [gate, up, down, col, hga, outs, fqa, ends, query, key, value, entry, decay]
    results = [proj, rows, rows, rows]
    return pl.pallas_call(
        tail_kernel,
        out_shape=tuple(shape(a.shape, a.dtype) for a in (gate, up, down)) + tuple(results),
        in_specs=[any_spec] * len(kept),
        out_specs=(any_spec,) * 7,
        scratch_shapes=[pltpu.VMEM(a.shape, a.dtype) for a in kept + results]
        + [pltpu.SemaphoreType.DMA((16,)), pltpu.SemaphoreType.DMA((16,))],
        compiler_params=pltpu.CompilerParams(vmem_limit_bytes=VMEM_LIMIT),
        cost_estimate=pl.CostEstimate(
            flops=2 * segs * count * quarter * channels,
            bytes_accessed=30000000,
            transcendentals=0,
        ),
    )(*kept)


def local_square(
    residual_mid,
    out_grad,
    norm_gain,
    expert_ids,
    expert_weights,
    gate_proj,
    up_proj,
    down_proj,
    out_proj,
    query_rows,
    key_rows,
    value_rows,
    retention_out,
    log_decay,
    entry_state,
):
    width = residual_mid.shape[1]
    segs = lax.axis_size("sp")
    gate_grad, up_grad, down_grad, columns, grads, outs, fqs, ends = square_call(
        segs,
        residual_mid,
        out_grad,
        expert_ids.T,
        expert_weights.T,
        log_decay.T,
        norm_gain.reshape(1, width),
        gate_proj[0],
        up_proj[0],
        down_proj[0],
        out_proj,
        retention_out,
        query_rows,
    )
    gate_grad, up_grad, down_grad, proj_grad, query_grad, key_grad, value_grad = tail_call(
        gate_grad,
        up_grad,
        down_grad,
        columns,
        grads.reshape(outs.shape),
        outs,
        fqs,
        ends,
        query_rows,
        key_rows,
        value_rows,
        entry_state[0],
        log_decay.T,
    )
    return (
        gate_grad[None],
        up_grad[None],
        down_grad[None],
        proj_grad,
        query_grad,
        key_grad,
        value_grad,
    )


def solution(mesh):
    segs, split = mesh.shape["sp"], mesh.shape["tp"]
    fine = Mesh(mesh.devices.reshape(segs, split // CORES, CORES), ("sp", "z", "core"))
    tp = ("z", "core")
    placed = (
        P("sp", None),
        P("sp", None),
        P(),
        P("sp", None),
        P("sp", None),
        P("sp", None, tp),
        P("sp", None, tp),
        P("sp", tp, None),
        P(tp, None),
        P("sp", tp),
        P("sp", tp),
        P("sp", tp),
        P("sp", tp),
        P("sp", tp),
        P("sp", tp, None, None),
    )
    fast = segs == 4 and split == segs * CORES
    return jax.shard_map(
        local_square if fast else local_general,
        mesh=fine,
        in_specs=placed,
        out_specs=(
            P("sp", None, tp),
            P("sp", None, tp),
            P("sp", tp, None),
            P("sp", tp),
            P("sp", tp),
            P("sp", tp),
            P("sp", tp),
        ),
        check_vma=False,
    )
```
